32 devices in a mesh: sp: 8 (over z, y), tp: 4 (over x, core).
Axes of the slice: x: 2, y: 2, z: 4, core: 2. Of those that a mesh axis runs over, the one named last changes fastest.
Arguments:
- cotangent: bfloat16 [1024, 2048], P('sp', 'tp'), may hold values from -6 to 6
- mixer_out: bfloat16 [1024, 2048], P('sp', 'tp'), may hold values from -6 to 6
- route_ids: int32 [1024, 2], P('sp'), may hold values from 0 to 7, all different within a row; in each aligned block of 128 rows (0 to 127, 128 to 255, ...) at most 64 rows name the same one
- route_weights: float32 [1024, 2], P('sp'), may hold values from 0.2 to 1
- conv_out: bfloat16 [1024, 2048], P('sp', 'tp'), may hold values from -6 to 6
- recur_gate: bfloat16 [1024, 2048], P('sp', 'tp'), may hold values from 0.007 to 1
- input_gate: bfloat16 [1024, 2048], P('sp', 'tp'), may hold values from 0.099609375 to 0.8984375
- gate_pre: bfloat16 [1024, 2048], P('sp', 'tp'), may hold values from -6 to 6
- states_before: bfloat16 [1024, 2048], P('sp', 'tp'), may hold values from -4 to 4
- decay_rate: float32 [2048], P('tp'), may hold values from 4e-07 to 0.008
- out_proj: bfloat16 [2048, 2048], P(None, 'tp'), may hold values from -0.125 to 0.125
- recur_map: bfloat16 [4, 512, 512], P('tp'), may hold values from -0.25 to 0.25
- input_map: bfloat16 [4, 512, 512], P('tp'), may hold values from -0.25 to 0.25
- expert_gate: bfloat16 [8, 2048, 1024], P('sp', None, 'tp'), may hold values from -0.125 to 0.125
- expert_up: bfloat16 [8, 2048, 1024], P('sp', None, 'tp'), may hold values from -0.125 to 0.125
- expert_down: bfloat16 [8, 1024, 2048], P('sp', 'tp'), may hold values from -0.1875 to 0.1875
Outputs:
- grad_expert_gate: bfloat16 [8, 2048, 1024], P('sp', None, 'tp')
- grad_expert_up: bfloat16 [8, 2048, 1024], P('sp', None, 'tp')
- grad_expert_down: bfloat16 [8, 1024, 2048], P('sp', 'tp')
- grad_out_proj: float32 [2048, 2048], P('sp', 'tp')
- grad_conv: bfloat16 [1024, 2048], P('sp', 'tp')
- grad_gate_pre: bfloat16 [1024, 2048], P('sp', 'tp')
The draws below stay inside these ranges and needn't reach their ends.
Inputs may be any that keep to these rules, and one draw needn't show every extreme that they name: `route_ids`: the two experts of a token differ. In every aligned block of 128 tokens no expert is named by more than 64 routes, and in some block some expert by exactly 64.
All inputs are finite; a program needn't handle non-finite values.
Results may differ from the reference program's by a relative error of at most 0.0093.
Values may be sent and summed in bfloat16 or wider, within the bound.
A program may use at most 64 MiB of HBM per device.

```python
import math
import jax
import jax.numpy as jnp
import numpy as np
from jax import lax

D = 2048
LRU = 2048
BLOCKS = 4
BLOCK_W = 512
FF = 1024
TOK_DEV = 128
TOKENS = 1024
EXPERTS = 8
CAP = 64
N_SP = 8


def draw_recur_gate(key, part):
    key_one, key_two = jax.random.split(key)
    span_count = TOKENS // 128
    base_gate = jax.random.uniform(key_one, (TOKENS, LRU), jnp.float32, 0.5, 1.0)
    factor = jnp.exp(jax.random.uniform(key_two, (span_count, 1, 1), jnp.float32, math.log(0.15), 0.0))
    return (base_gate.reshape(span_count, 128, LRU) * factor).reshape(TOKENS, LRU).astype(jnp.bfloat16)


def draw_decay_rate(key, part):
    key_one, key_two, key_three = jax.random.split(key, 3)
    fast_share = 0.5
    fast_mask = jax.random.bernoulli(key_one, fast_share, (LRU,))
    slow_rate = jnp.exp(jax.random.uniform(key_two, (LRU,), jnp.float32, math.log(0.03), math.log(0.25))) / TOKENS
    fast_rate = jnp.exp(jax.random.uniform(key_three, (LRU,), jnp.float32, math.log(0.002), math.log(0.008)))
    return jnp.where(fast_mask, fast_rate, slow_rate).astype(jnp.float32)


def with_spikes(entries, own_key, source, target, shards_of, factor):
    owner, partner = [(jnp.arange(entries.shape[axis_at]) // (entries.shape[axis_at] // shards_of)).reshape([-1 if axis == axis_at else 1 for axis in range(entries.ndim)]) for axis_at in (source, target)]
    chosen = jax.random.permutation(own_key, shards_of)[partner]
    strong = (owner == chosen) | (owner == (partner + shards_of // 2) % shards_of)
    return jnp.where(strong, factor * entries, entries)


def steps_of(own_key, extent, cuts, smallest, largest):
    level, own = 1.0, jax.random.fold_in(own_key, 6)
    for position, parts in cuts:
        steps = jnp.exp(jax.random.uniform(jax.random.fold_in(own, position), (parts,), jnp.float32, smallest / len(cuts), largest / len(cuts)))
        level = level * jnp.repeat(steps, extent[position] // parts).reshape([-1 if axis == position else 1 for axis in range(len(extent))])
    return level


def shared_out(rng, own, number, rows, number_of, top, reach, skew):
    order = jax.random.permutation(rng, number_of)
    packed, ordinary = load_shares(number_of, rows * top, reach, skew, True), load_shares(number_of, rows * top, reach, skew, False)
    places = jnp.arange(number_of)

    def named(tallies, turn):
        used = int((tallies > 0).sum())
        fixed = max(1, used // 4)
        moved = fixed + (places - fixed + turn * (used - fixed)) % max(1, number_of - fixed)
        return jnp.zeros((number_of,), jnp.int32).at[order[jnp.where(places < fixed, places, moved)]].set(jnp.asarray(tallies, jnp.int32))

    tallies = jnp.where(number % 4 == 0, named(packed, number // 4), named(ordinary, number - number // 4 - 1))
    mixed = jax.random.permutation(jax.random.fold_in(own, 3), number_of)
    donor, taker = mixed[0:number_of // 2 * 2:2], mixed[1:number_of // 2 * 2:2]
    margin = jnp.minimum(tallies[donor] - 1, reach - tallies[taker]) // 2
    margin = jnp.where((donor == order[0]) | (taker == order[0]) | (tallies[taker] == 0), 0, jnp.maximum(margin, 0))
    moved = jax.random.randint(jax.random.fold_in(own, 4), (number_of // 2,), 0, 1 << 20) % (margin + 1)
    tallies = tallies.at[donor].add(-moved).at[taker].add(moved)
    items = jnp.searchsorted(jnp.cumsum(tallies), jnp.arange(rows * top), side="right").astype(jnp.int32)
    listing = items.reshape(top, rows).T
    listing = listing[jax.random.permutation(jax.random.fold_in(own, 1), rows)]
    turn = jax.random.randint(jax.random.fold_in(own, 2), (rows, 1), 0, top)
    return jnp.take_along_axis(listing, (jnp.arange(top)[None, :] + turn) % top, axis=1)


def load_shares(amount, total, limit, lean, full):
    loads = [(1 << 20) // math.isqrt(standing ** lean) + 1 for standing in range(1, amount + 1)]
    largest = limit if full else min(limit, max(-(-total // amount), total * loads[0] // sum(loads)))
    least = 1 if total - largest >= amount - 1 else 0
    given, rest = [largest] + [least] * (amount - 1), total - largest - least * (amount - 1)
    while rest > 0:
        free = [i for i in range(1, amount) if given[i] < largest] or [i for i in range(1, amount) if given[i] < limit]
        mass, left = sum([loads[i] for i in free]), rest
        for i in free:
            extra = min(limit - given[i], max(1, left * loads[i] // mass), rest)
            given[i] = given[i] + extra
            rest = rest - extra
    return np.array(given)


def scatter_about(stream_key, dims, deviation, reach, cuts=(), held_as=jnp.bfloat16):
    loudness = steps_of(stream_key, dims, cuts, -0.22, 0.18) if cuts else 1.0
    values = jax.random.normal(stream_key, dims, jnp.float32) * deviation * loudness
    return jnp.minimum(jnp.maximum(values, -reach), reach).astype(held_as)


def noise_with(own_key, dims, width, reach, shards, heavy, kind=jnp.bfloat16):
    array = width * jax.random.normal(own_key, dims, jnp.float32)
    if shards:
        array = array * steps_of(own_key, dims, shards, -0.22, 0.18)
    return jnp.clip(with_spikes(array, jax.random.fold_in(own_key, 3), *heavy), -reach, reach).astype(kind)


def setup_inputs(seed: int = 0) -> dict:
    key_list = jax.random.split(jax.random.key(seed), 17)
    cotangent = noise_with(key_list[0], (TOKENS, D), 1.0, 6.0, ((0, 8), (1, 4)), (0, 1, 8, 2.0))
    mixer_out = scatter_about(key_list[1], (TOKENS, D), 1.0, 6.0, ((0, 8), (1, 4)))
    route_ids_keys = jax.random.split(jax.random.fold_in(key_list[2], 1), TOKENS // TOK_DEV)
    route_ids_turns = jax.random.permutation(jax.random.fold_in(key_list[2], 3), TOKENS // TOK_DEV)
    route_ids = jax.vmap(lambda own, number: shared_out(jax.random.fold_in(key_list[2], 2), own, number, TOK_DEV, EXPERTS, 2, CAP, 2))(route_ids_keys, route_ids_turns).reshape((TOKENS, 2))
    route_weights = jnp.clip(0.2 + 0.8 * jax.random.uniform(key_list[3], (TOKENS, 2), jnp.float32) ** steps_of(key_list[3], (TOKENS, 2), ((0, 8),), -0.2, 0.2), 0.2, 1.0)
    conv_out = scatter_about(key_list[4], (TOKENS, LRU), 1.0, 6.0, ((0, 8), (1, 4)))
    recur_gate = draw_recur_gate(jax.random.fold_in(key_list[16], 71), 0)
    input_gate = jnp.clip(0.099609375 + 0.7988281 * jax.random.uniform(key_list[6], (TOKENS, LRU), jnp.float32) ** steps_of(key_list[6], (TOKENS, LRU), ((0, 8), (1, 4)), -0.2, 0.2), 0.099609375, 0.8984375).astype(jnp.bfloat16)
    gate_pre = scatter_about(key_list[7], (TOKENS, LRU), 1.0, 6.0, ((0, 8), (1, 4)))
    states_before = scatter_about(key_list[8], (TOKENS, LRU), 0.5, 4.0, ((0, 8), (1, 4)))
    decay_rate = draw_decay_rate(jax.random.fold_in(key_list[16], 71), 0)
    out_proj = scatter_about(key_list[10], (D, LRU), LRU ** -0.5, 0.125, ((1, 4),))
    recur_map = scatter_about(key_list[11], (BLOCKS, BLOCK_W, BLOCK_W), BLOCK_W ** -0.5, 0.25, ((0, 4),))
    input_map = scatter_about(key_list[12], (BLOCKS, BLOCK_W, BLOCK_W), BLOCK_W ** -0.5, 0.25, ((0, 4),))
    expert_gate = scatter_about(key_list[13], (EXPERTS, D, FF), D ** -0.5, 0.125, ((0, 8), (2, 4)))
    expert_up = scatter_about(key_list[14], (EXPERTS, D, FF), D ** -0.5, 0.125, ((0, 8), (2, 4)))
    expert_down = scatter_about(key_list[15], (EXPERTS, FF, D), FF ** -0.5, 0.1875, ((0, 8), (1, 4)))
    return dict(cotangent=cotangent, mixer_out=mixer_out, route_ids=route_ids, route_weights=route_weights, conv_out=conv_out, recur_gate=recur_gate, input_gate=input_gate, gate_pre=gate_pre, states_before=states_before, decay_rate=decay_rate, out_proj=out_proj, recur_map=recur_map, input_map=input_map, expert_gate=expert_gate, expert_up=expert_up, expert_down=expert_down)


def silu_parts(values):
    sig = jax.nn.sigmoid(values)
    return (values * sig, sig * (1.0 + values * (1.0 - sig)))

def route_slots(route_block):
    flat_ids = route_block.reshape(-1)
    onehot = (flat_ids[:, None] == jnp.arange(EXPERTS, dtype=jnp.int32)[None, :]).astype(jnp.int32)
    before = jnp.cumsum(onehot, axis=0) - onehot
    slot_rank = lax.optimization_barrier(jnp.sum(before * onehot, axis=1))
    return (flat_ids * CAP + slot_rank).astype(jnp.int32)

def link_steps(earlier, later):
    return (earlier[0] * later[0], later[0] * earlier[1] + later[1])

def reference(cotangent, mixer_out, route_ids, route_weights, conv_out, recur_gate, input_gate, gate_pre, states_before, decay_rate, out_proj, recur_map, input_map, expert_gate, expert_up, expert_down):
    slot_pos = jax.vmap(route_slots)(route_ids.reshape(N_SP, TOK_DEV, 2))
    expert_of = slot_pos // CAP
    slot_rank = slot_pos % CAP
    source = jnp.arange(N_SP, dtype=jnp.int32)[:, None]
    place = (expert_of * (N_SP * CAP) + source * CAP + slot_rank).astype(jnp.int32).reshape(-1)
    token_of = (source * TOK_DEV + jnp.arange(2 * TOK_DEV, dtype=jnp.int32)[None, :] // 2).astype(jnp.int32)
    table = jnp.full((EXPERTS * N_SP * CAP,), TOKENS, jnp.int32).at[place].set(token_of.reshape(-1))
    slot_weight = jnp.zeros((EXPERTS * N_SP * CAP,), jnp.float32).at[place].set(route_weights.astype(jnp.float32).reshape(-1))
    table = table.reshape(EXPERTS, N_SP * CAP)
    slot_weight = slot_weight.reshape(EXPERTS, N_SP * CAP)
    x_padded = jnp.concatenate([mixer_out, jnp.zeros((1, D), jnp.bfloat16)], axis=0)
    g_padded = jnp.concatenate([cotangent, jnp.zeros((1, D), jnp.bfloat16)], axis=0)

    def expert_step(routed_sum, inputs):
        row_index, weight, w_gate, w_up, w_down = inputs
        row_data = x_padded[row_index]
        routed_cot = (g_padded[row_index].astype(jnp.float32) * weight[:, None]).astype(jnp.bfloat16)
        pre_gate = jnp.dot(row_data, w_gate, preferred_element_type=jnp.float32)
        pre_up = jnp.dot(row_data, w_up, preferred_element_type=jnp.float32)
        gate_act, slope = silu_parts(pre_gate)
        active = (gate_act * pre_up).astype(jnp.bfloat16)
        d_active = jnp.dot(routed_cot, w_down.T, preferred_element_type=jnp.float32)
        grad_down = jnp.dot(active.T, routed_cot, preferred_element_type=jnp.float32).astype(jnp.bfloat16)
        d_gate = (d_active * pre_up * slope).astype(jnp.bfloat16)
        d_up = (d_active * gate_act).astype(jnp.bfloat16)
        grad_gate = jnp.dot(row_data.T, d_gate, preferred_element_type=jnp.float32).astype(jnp.bfloat16)
        grad_up = jnp.dot(row_data.T, d_up, preferred_element_type=jnp.float32).astype(jnp.bfloat16)
        route_grad = (jnp.dot(d_gate, w_gate.T, preferred_element_type=jnp.float32) + jnp.dot(d_up, w_up.T, preferred_element_type=jnp.float32)).astype(jnp.bfloat16)
        routed_sum = routed_sum.at[row_index].add(route_grad.astype(jnp.float32))
        return (routed_sum, (grad_gate, grad_up, grad_down))
    routed_sum, expert_grads = lax.scan(expert_step, jnp.zeros((TOKENS + 1, D), jnp.float32), (table, slot_weight, expert_gate, expert_up, expert_down))
    grad_expert_gate, grad_expert_up, grad_expert_down = expert_grads
    out_grad = (cotangent.astype(jnp.float32) + routed_sum[:TOKENS]).astype(jnp.bfloat16)
    rate = decay_rate.astype(jnp.float32)[None, :]
    recur_f = recur_gate.astype(jnp.float32)
    input_f = input_gate.astype(jnp.float32)
    conv_f = conv_out.astype(jnp.float32)
    before_f = states_before.astype(jnp.float32)
    log_decay = -8.0 * recur_f * rate
    decay_now = jnp.exp(log_decay)
    at_start = (jnp.arange(TOKENS, dtype=jnp.int32) == 0)[:, None]
    norm_factor = jnp.where(at_start, 1.0, jnp.sqrt(-jnp.expm1(2.0 * log_decay)))
    norm_slope = jnp.where(at_start, 0.0, -jnp.exp(2.0 * log_decay) / norm_factor)
    drive = input_f * conv_f
    state = decay_now * before_f + norm_factor * drive
    gate, gelu_back = jax.vjp(jax.nn.gelu, gate_pre.astype(jnp.float32))
    mixed = (state * gate).astype(jnp.bfloat16)
    d_mixed = jnp.dot(out_grad, out_proj, preferred_element_type=jnp.float32)
    grad_out_proj = jnp.dot(out_grad.T, mixed, preferred_element_type=jnp.float32)
    grad_gate_pre = gelu_back(d_mixed * state)[0].astype(jnp.bfloat16)
    decay_next = jnp.concatenate([decay_now[1:], jnp.ones((1, LRU), jnp.float32)], axis=0)
    _, state_grad = lax.associative_scan(link_steps, (decay_next, d_mixed * gate), axis=0, reverse=True)
    d_log = state_grad * (decay_now * before_f + norm_slope * drive)
    d_recur_pre = (d_log * (-8.0 * rate) * recur_f * (1.0 - recur_f)).astype(jnp.bfloat16)
    d_input_pre = (state_grad * norm_factor * conv_f * input_f * (1.0 - input_f)).astype(jnp.bfloat16)
    through_recur = jnp.einsum('tbj,bij->tbi', d_recur_pre.astype(jnp.float32).reshape(TOKENS, BLOCKS, BLOCK_W), recur_map.astype(jnp.float32))
    through_input = jnp.einsum('tbj,bij->tbi', d_input_pre.astype(jnp.float32).reshape(TOKENS, BLOCKS, BLOCK_W), input_map.astype(jnp.float32))
    grad_conv = (state_grad * norm_factor * input_f + (through_recur + through_input).reshape(TOKENS, LRU)).astype(jnp.bfloat16)
    return (grad_expert_gate, grad_expert_up, grad_expert_down, grad_out_proj, grad_conv, grad_gate_pre)
```

```python
import functools

import jax
import jax.numpy as jnp
from jax import lax
from jax.experimental import pallas as pl
from jax.experimental.pallas import tpu as pltpu
from jax.sharding import PartitionSpec as P

MESH = pl.DeviceIdType.MESH
VMEM = pl.BlockSpec(memory_space=pltpu.VMEM)
DMA = pltpu.SemaphoreType.DMA


def bits_of(count):
    found, bit = [], 1
    while bit < count:
        found.insert(0, bit)
        bit *= 2
    return found


def low_bit(mask):
    return mask & -mask


def flip(index, mask):
    bit = 1
    while bit <= mask:
        if mask & bit:
            index = index + bit - 2 * bit * lax.rem(lax.div(index, bit), 2)
        bit *= 2
    return index


def window(index, width):
    return pl.ds(pl.multiple_of(index * width, width), width)


def remote(source, target, send_sem, recv_sem, device):
    return pltpu.make_async_remote_copy(
        src_ref=source,
        dst_ref=target,
        send_sem=send_sem,
        recv_sem=recv_sem,
        device_id=device,
        device_id_type=MESH,
    )


def greet(peers):
    barrier = pltpu.get_barrier_semaphore()
    for peer in peers:
        pl.semaphore_signal(barrier, inc=1, device_id=peer, device_id_type=MESH)
    pl.semaphore_wait(barrier, len(peers))


def relays_of(count):
    masks = [mask for mask in range(1, count) if mask != low_bit(mask)]
    return sorted(masks, key=lambda mask: (bin(mask).count("1"), -mask))


def call(kernel, out_shape, scratch, ident, *operands):
    return pl.pallas_call(
        kernel,
        out_shape=out_shape,
        in_specs=[VMEM] * len(operands),
        out_specs=jax.tree.map(lambda _: VMEM, out_shape),
        scratch_shapes=scratch,
        compiler_params=pltpu.CompilerParams(
            collective_id=ident, has_side_effects=True, vmem_limit_bytes=48 * 1024 * 1024
        ),
    )(*operands)


def along(index, table):
    found = 0
    for place, value in enumerate(table):
        found = found + jnp.where(index == place, value, 0)
    return found


def abs_of(value):
    return jnp.where(value < 0, -value, value)


def nearest(count):
    return [sorted(range(count), key=lambda other: (abs(other - z), other)) for z in range(count)]


def contract_columns(left, right):
    return lax.dot_general(
        left, right, (((1,), (1,)), ((), ())), preferred_element_type=jnp.float32
    )


def expm1_of(values):
    near = 1.0 / 362880.0
    for factor in (40320.0, 5040.0, 720.0, 120.0, 24.0, 6.0, 2.0, 1.0):
        near = near * values + 1.0 / factor
    return jnp.where(jnp.abs(values) < 0.3, values * near, jnp.exp(values) - 1.0)


def expert_kernel(
    n_sp, n_tp, capacity,
    rows_hbm, cots_hbm, ids_hbm, weights_hbm, conv_hbm, recur_hbm, input_hbm, gate_hbm,
    before_hbm, rate_hbm, proj_hbm, w_gate_hbm, w_up_hbm, w_down_hbm,
    mixed_all, pieces, grad_gate, grad_up, grad_down, state_grad, recur_part, input_part,
    conv_part, grad_gate_pre,
    rows, cots, ids, weights, conv, recur, inputs, gate_pre, before, rate, proj,
    w_gate, w_up, w_down,
    tok, meta, got, ybuf, act, dgate, dup, give_pair, mine, half,
    xsend, xrecv, back, ret, pick, out, mixed, decay, gate, gate_part, drive, product, carry,
    carries,
    lsem, tss, trs, mss, mrs, yss, yrs, hss, hrs, pss, prs, css, crs, gss, grs,
    zss, zrs, oss, ors, iss, irs, kss, krs, own_sem,
):
    s, t = lax.axis_index("sp"), lax.axis_index("tp")
    n_y = 2
    n_z = n_sp // n_y
    z, y = lax.div(s, n_y), lax.rem(s, n_y)
    beside = flip(s, 1)
    pair, across = flip(t, 1), flip(t, 2)
    tokens, width = rows.shape
    chunk = n_y * capacity
    f32, bf16 = jnp.float32, jnp.bfloat16
    order = [along(z, [found[k] for found in nearest(n_z)]) for k in range(n_z)]

    fetch = [
        pltpu.make_async_copy(source, target, lsem.at[i])
        for i, (source, target) in enumerate(
            (
                (rows_hbm, rows), (cots_hbm, cots), (ids_hbm, ids), (weights_hbm, weights),
                (conv_hbm, conv), (recur_hbm, recur), (input_hbm, inputs), (gate_hbm, gate_pre),
                (before_hbm, before), (rate_hbm, rate),
                (w_gate_hbm, w_gate), (w_up_hbm, w_up), (w_down_hbm, w_down), (proj_hbm, proj),
            )
        )
    ]
    for copy in fetch:
        copy.start()
    barrier_peers = [(flip(s, m), t) for m in range(1, n_sp)]
    barrier_peers += [(flip(s, m), flip(t, 2)) for m in range(1, n_sp)]
    greet(barrier_peers + [(s, flip(t, b)) for b in bits_of(n_tp)])
    for copy in fetch[:4]:
        copy.wait()
    ends = []

    def begin(copy, valid=None):
        ends.append((copy, valid))
        if valid is None:
            copy.start()
        else:
            pl.when(valid)(copy.start)

    def spread(make, zb, first):
        above, below = z + 1 < n_z, z >= 1
        if not first:
            above, below = (zb < z) & above, (zb > z) & below
        begin(make(zb, z + 1, 0), above)
        begin(make(zb, z - 1, 1), below)

    def along_line(source, target, send_sem, recv_sem, z_to):
        return remote(source, target, send_sem, recv_sem, (z_to * n_y + y, t))

    def move_tokens(kind, zb, z_to, way, own):
        target = tok.at[kind, zb]
        source = (rows, cots)[kind] if own else target
        return along_line(source, target, tss.at[kind, zb, way], trs.at[kind, zb], z_to)

    def move_meta(zb, z_to, way):
        return along_line(meta.at[zb], meta.at[zb], mss.at[zb, way], mrs.at[zb], z_to)

    def move_mixed(zb, z_to, way, own):
        target = mixed_all.at[zb * n_y + y]
        source = mixed if own else target
        return along_line(source, target, zss.at[zb, way], zrs.at[zb * n_y + y], z_to)

    def mixed_beside(zb, own):
        target = mixed_all.at[zb * n_y + y]
        source = mixed if own else target
        return remote(source, target, zss.at[zb, 2], zrs.at[zb * n_y + y], (beside, t))

    def mixed_from_beside(zb):
        target = mixed_all.at[zb * n_y + 1 - y]
        return remote(mixed, target, zss.at[zb, 2], zrs.at[zb * n_y + 1 - y], (beside, t))

    def slots(kind, block, quarter):
        return got.at[kind, window(block, capacity), window(quarter, width)]

    def to_beside(kind, zb):
        return remote(
            ybuf.at[kind, zb], slots(kind, zb * n_y + y, t),
            yss.at[kind, zb], yrs.at[kind, zb], (beside, t),
        )

    def from_beside(kind, zb):
        return remote(
            ybuf.at[kind, zb], slots(kind, zb * n_y + 1 - y, t),
            yss.at[kind, zb], yrs.at[kind, zb], (beside, t),
        )

    def share(kind, block, k):
        bit = low_bit(k)
        ref = slots(kind, block, flip(t, k - bit))
        return remote(ref, ref, hss.at[kind, block, k], hrs.at[kind, block, k], (s, flip(t, bit)))

    def arrived(kind, block, k):
        ref = slots(kind, block, flip(t, k))
        return remote(
            ref, ref, hss.at[kind, block, k], hrs.at[kind, block, k], (s, flip(t, low_bit(k)))
        )

    table_rows = lax.broadcasted_iota(jnp.int32, (2 * n_sp, tokens), 0)
    first_id, second_id = ids[0:1, :], ids[1:2, :]
    hits = ((first_id == table_rows) | (second_id == table_rows)).astype(f32)
    earlier = lax.broadcasted_iota(jnp.int32, (tokens, tokens), 0) < lax.broadcasted_iota(
        jnp.int32, (tokens, tokens), 1
    )
    rank = jnp.dot(
        hits.astype(bf16), earlier.astype(f32).astype(bf16), preferred_element_type=f32
    )
    rank = jnp.where(hits > 0.0, rank, -1.0)
    weight_rows = table_rows - n_sp
    weight = jnp.where(first_id == weight_rows, weights[0:1, :], 0.0) + jnp.where(
        second_id == weight_rows, weights[1:2, :], 0.0
    )
    meta[z] = jnp.where(table_rows < n_sp, rank, weight)

    spread(lambda zb, to, way: move_tokens(0, zb, to, way, True), z, True)
    spread(move_meta, z, True)
    spread(lambda zb, to, way: move_tokens(1, zb, to, way, True), z, True)

    slot_index = lax.broadcasted_iota(jnp.int32, (capacity, tokens), 0).astype(f32)

    def chosen(zb, expert):
        return meta[zb, pl.ds(expert, 1), :] == slot_index

    def compact(kind, k, valid=None):
        zb = order[k]
        block = zb * n_y + y
        sends = (to_beside(kind, zb), share(kind, block, 2), share(kind, block, 1))
        ends.extend((copy, valid) for copy in sends)

        def work():
            picks = jnp.concatenate(
                [chosen(zb, s).astype(f32), chosen(zb, beside).astype(f32)], axis=0
            )
            source = tok[kind, zb] if k > 0 else (rows, cots)[kind][...]
            found = jnp.dot(picks.astype(bf16), source, preferred_element_type=f32)
            if kind == 1:
                table = jnp.concatenate(
                    [
                        jnp.broadcast_to(meta[zb, pl.ds(n_sp + e, 1), :], (capacity, tokens))
                        for e in (s, beside)
                    ],
                    axis=0,
                )
                found = found * jnp.sum(picks * table, axis=1, keepdims=True)
            found = found.astype(bf16)
            ybuf[kind, zb] = found[capacity:]
            got[kind, window(block, capacity), window(t, width)] = found[:capacity]
            for copy in sends:
                copy.start()

        if valid is None:
            work()
        else:
            pl.when(valid)(work)

    def hear(distance, kind):
        for k in range(1, n_z):
            apart = {abs(found[k] - place) for place, found in enumerate(nearest(n_z))}
            if distance not in apart:
                continue
            zb = order[k]
            only = None if len(apart) == 1 else abs_of(zb - z) == distance
            waits = [move_tokens(kind, zb, z, 0, False)] + [move_meta(zb, z, 0)] * (kind == 0)
            for copy in waits:
                if only is None:
                    copy.wait_recv()
                else:
                    pl.when(only)(copy.wait_recv)
            make = [lambda zb, to, way: move_tokens(kind, zb, to, way, False)]
            for made in make + [move_meta] * (kind == 0):
                above, below = (zb < z) & (z + 1 < n_z), (zb > z) & (z >= 1)
                if only is not None:
                    above, below = above & only, below & only
                begin(made(zb, z + 1, 0), above)
                begin(made(zb, z - 1, 1), below)
        for k in range(1, n_z):
            apart = {abs(found[k] - place) for place, found in enumerate(nearest(n_z))}
            if distance in apart:
                only = None if len(apart) == 1 else abs_of(order[k] - z) == distance
                compact(kind, k, only)

    def take_beside(kind, k):
        block = order[k] * n_y + 1 - y
        from_beside(kind, order[k]).wait_recv()
        begin(share(kind, block, 2))
        begin(share(kind, block, 1))

    def gather_chunk(k):
        blocks = [order[k] * n_y + y, order[k] * n_y + 1 - y]
        for block in blocks:
            for kind in range(2):
                arrived(kind, block, 2).wait_recv()
                begin(share(kind, block, 3))
        for block in blocks:
            for kind in range(2):
                arrived(kind, block, 1).wait_recv()
                arrived(kind, block, 3).wait_recv()

    def to_pair(zb, slot):
        here = window(zb, chunk)
        return remote(
            give_pair.at[slot, here], half.at[slot, here],
            pss.at[zb, slot], prs.at[zb, slot], (s, pair),
        )

    def cross(zb):
        here = window(zb, chunk)
        return remote(xsend.at[here], xrecv.at[here], css.at[zb], crs.at[zb], (s, across))

    def give(block):
        here = window(block, capacity)
        return remote(
            back.at[here], ret.at[window(s, capacity)], gss.at[block], grs.at[s], (block, t)
        )

    def given(source):
        here = window(source, capacity)
        return remote(back.at[here], ret.at[here], gss.at[source], grs.at[source], (source, t))

    def experts(k):
        zb = order[k]
        here = window(zb, chunk)
        got_rows = got[0, here, :]
        pre_gate = jnp.dot(got_rows, w_gate[...], preferred_element_type=f32)
        pre_up = jnp.dot(got_rows, w_up[...], preferred_element_type=f32)
        d_active = contract_columns(got[1, here, :], w_down[...])
        gate_act, slope = silu_parts(pre_gate)
        act[here, :] = (gate_act * pre_up).astype(bf16)
        d_gate = (d_active * pre_up * slope).astype(bf16)
        d_up = (d_active * gate_act).astype(bf16)
        dgate[here, :] = d_gate
        dup[here, :] = d_up

        def partial(quarter):
            columns = window(quarter, width)
            return contract_columns(d_gate, w_gate[columns, :]) + contract_columns(
                d_up, w_up[columns, :]
            )

        give_pair[0, here, :] = partial(flip(pair, 2)).astype(bf16)
        begin(to_pair(zb, 0))
        give_pair[1, here, :] = partial(pair).astype(bf16)
        begin(to_pair(zb, 1))
        mine[0, here, :] = partial(across)
        mine[1, here, :] = partial(t)

    def send_across(k):
        zb = order[k]
        here = window(zb, chunk)
        to_pair(zb, 0).wait_recv()
        xsend[here, :] = (mine[0, here, :] + half[0, here, :].astype(f32)).astype(bf16)
        begin(cross(zb))

    def send_home(k):
        zb = order[k]
        here = window(zb, chunk)
        to_pair(zb, 1).wait_recv()
        cross(zb).wait_recv()
        total = (
            mine[1, here, :] + half[1, here, :].astype(f32) + xrecv[here, :].astype(f32)
        ).astype(bf16)
        back[here, :] = total
        if k > 0:
            begin(give(zb * n_y + y))
        else:
            ret[window(s, capacity), :] = back[window(s, capacity), :]
        begin(give(zb * n_y + 1 - y))

    step = 256 if width % 256 == 0 else width

    def weight_grad(target, kind, right):
        def lap(j, _):
            columns = window(j, step)
            target[columns, :] = contract_rows(got[kind, :, columns], right[...]).astype(bf16)
            return 0

        lax.fori_loop(0, n_tp * width // step, lap, 0)

    def down_grad():
        def lap(j, _):
            columns = window(j, step)
            grad_down[:, columns] = contract_rows(act[...], got[1, :, columns]).astype(bf16)
            return 0

        lax.fori_loop(0, n_tp * width // step, lap, 0)

    def take_mixed(k):
        zb = order[k]
        if k == 0:
            spread(lambda zb, to, way: move_mixed(zb, to, way, True), zb, True)
        else:
            move_mixed(zb, z, 0, False).wait_recv()
            spread(lambda zb, to, way: move_mixed(zb, to, way, False), zb, False)
        begin(mixed_beside(zb, k == 0))

    def share_out(k):
        bit = low_bit(k)
        ref = out.at[:, window(flip(t, k - bit), width)]
        return remote(ref, ref, oss.at[k], ors.at[k], (s, flip(t, bit)))

    def out_arrived(k):
        ref = out.at[:, window(flip(t, k), width)]
        return remote(ref, ref, oss.at[k], ors.at[k], (s, flip(t, low_bit(k))))

    strip = 16

    def recurrence():
        def lap(j, _):
            here = window(j, strip)
            rate_row = rate[...]
            recur_f = recur[here, :].astype(f32)
            input_f = inputs[here, :].astype(f32)
            conv_f = conv[here, :].astype(f32)
            before_f = before[here, :].astype(f32)
            gate_f = gate_pre[here, :].astype(f32)
            log_decay = -8.0 * recur_f * rate_row
            decay_now = jnp.exp(log_decay)
            place = lax.broadcasted_iota(jnp.int32, conv_f.shape, 0) + (s * tokens + j * strip)
            at_start = place == 0
            norm = jnp.where(at_start, 1.0, jnp.sqrt(-expm1_of(2.0 * log_decay)))
            slope = jnp.where(at_start, 0.0, -jnp.exp(2.0 * log_decay) / norm)
            entry = input_f * conv_f
            kept = decay_now * before_f
            state = kept + norm * entry
            inner = 0.7978845608028654 * (gate_f + 0.044715 * gate_f * gate_f * gate_f)
            bend = jnp.tanh(inner)
            half_up = 0.5 * (1.0 + bend)
            gate_now = gate_f * half_up
            gate_slope = half_up + 0.5 * gate_f * (1.0 - bend * bend) * 0.7978845608028654 * (
                1.0 + 3.0 * 0.044715 * gate_f * gate_f
            )
            decay[here, :] = decay_now
            gate[here, :] = gate_now
            gate_part[here, :] = state * gate_slope
            mixed[here, :] = (state * gate_now).astype(bf16)
            recur_part[here, :] = (
                (kept + slope * entry) * (-8.0 * rate_row) * recur_f * (1.0 - recur_f)
            )
            input_part[here, :] = norm * conv_f * input_f * (1.0 - input_f)
            conv_part[here, :] = norm * input_f
            return 0

        lax.fori_loop(0, tokens // strip, lap, 0)

        def back_lap(step, held):
            row = tokens - 1 - step
            product[pl.ds(row, 1), :] = held
            return held * decay[pl.ds(row, 1), :]

        one = jnp.ones((1, width), f32)
        carry[0:1, :] = lax.fori_loop(0, tokens, back_lap, one, unroll=8)

    cut = n_tp * width // n_sp
    held_blocks = width // cut

    def piece(q, t_to):
        columns = window(q, cut)
        return remote(
            out.at[:, columns], pieces.at[s], iss.at[q, lax.div(t_to, 2)], irs.at[s], (q, t_to)
        )

    def piece_beside(block):
        return remote(
            pieces.at[block], pieces.at[block], kss.at[block], irs.at[block], (s, pair)
        )

    def send_carry(m):
        return remote(carry, carries.at[s], krs.at[0, m], krs.at[1, m], (flip(s, m), t))

    for kind in range(2):
        compact(kind, 0)
    for expert in range(n_sp):
        pick[expert * capacity : (expert + 1) * capacity, :] = (
            chosen(z, expert).astype(f32).astype(bf16)
        )
    for kind in range(2):
        take_beside(kind, 0)
    for distance in range(1, n_z):
        hear(distance, 0)
        if distance == 1:
            hear(distance, 1)
            take_beside(0, 1)
            for copy in fetch[4:]:
                copy.wait()
            recurrence()
            own_mixed = pltpu.make_async_copy(mixed, mixed_all.at[s], own_sem)
            own_mixed.start()
            continue
        take_beside(1, distance - 1)
        gather_chunk(distance - 2)
        experts(distance - 2)
        hear(distance, 1)
        take_beside(0, distance)
    take_mixed(0)
    take_beside(1, n_z - 1)
    for k in range(n_z - 2, n_z):
        gather_chunk(k)
        experts(k)
        if k < n_z - 1:
            take_mixed(1)
        if k == n_z - 2:
            for earlier_k in range(1, n_z - 1):
                send_across(earlier_k)
    send_across(n_z - 1)
    send_across(0)
    for k in range(2, n_z):
        take_mixed(k)
    for k in range(1, n_z - 1):
        send_home(k)
    down_grad()
    send_home(n_z - 1)
    weight_grad(grad_gate, 0, dgate)
    send_home(0)
    weight_grad(grad_up, 0, dup)
    for m in range(1, n_sp):
        given(flip(s, m)).wait_recv()
    total = cots[...].astype(f32) + contract_rows(pick[...], ret[...])
    out[:, window(t, width)] = total.astype(bf16)
    begin(share_out(2))
    begin(share_out(1))
    for j in range(held_blocks):
        q = t * held_blocks + j
        begin(piece(q, t), abs_of(q - s) > 0)
        begin(piece(q, across), abs_of(q - s) > 0)

    def through_proj(k):
        columns = window(flip(t, k), width)
        return jnp.dot(out[:, columns], proj[columns, :], preferred_element_type=f32)

    drive[...] = through_proj(0)
    out_arrived(1).wait_recv()
    drive[...] += through_proj(1)
    out_arrived(2).wait_recv()
    begin(share_out(3))
    drive[...] += through_proj(2)
    out_arrived(3).wait_recv()
    d_mixed = drive[...] + through_proj(3)
    grad_gate_pre[...] = (d_mixed * gate_part[...]).astype(bf16)
    drive[...] = d_mixed * gate[...]

    def lap(step, held):
        row = tokens - 1 - step
        grad = drive[pl.ds(row, 1), :] + held
        state_grad[pl.ds(row, 1), :] = grad
        return decay[pl.ds(row, 1), :] * grad

    zero = jnp.zeros((1, width), f32)
    carry[1:2, :] = lax.fori_loop(0, tokens, lap, zero, unroll=8)
    for m in range(1, n_sp):
        begin(send_carry(m))
    own_piece = out[:, window(s, cut)]
    pieces[s] = own_piece
    direct = lax.rem(lax.div(s, held_blocks), 2) == lax.rem(t, 2)
    for m in range(1, n_sp):
        block = flip(s, m)
        pl.when(direct)(piece_beside(block).wait_recv)
        begin(piece_beside(block), direct)
    for m in range(1, n_sp):
        send_carry(m).wait_recv()
    incoming = zero
    for later in range(n_sp - 1, 0, -1):
        longer = carries[later, 1:2, :] + carries[later, 0:1, :] * incoming
        incoming = jnp.where(later > s, longer, incoming)
    state_grad[...] = state_grad[...] + product[...] * incoming
    for m in range(1, n_sp):
        pl.when(jnp.logical_not(direct))(piece_beside(flip(s, m)).wait_recv)
    for k in range(n_z):
        mixed_from_beside(order[k]).wait_recv()
    own_mixed.wait()
    for copy, valid in ends:
        if valid is None:
            copy.wait_send()
        else:
            pl.when(valid)(copy.wait_send)


def finish_kernel(
    mixed_all, pieces, grad_gate, grad_up, grad_down, state_grad, recur_part, input_part,
    conv_part, grad_gate_pre, recur_hbm, input_hbm,
    out_gate, out_up, out_down, out_proj, out_conv, out_gate_pre,
    recur_map, input_map, proj_block, conv_block, sems,
):
    loads = [
        pltpu.make_async_copy(recur_hbm, recur_map, sems.at[0]),
        pltpu.make_async_copy(input_hbm, input_map, sems.at[1]),
    ]
    for copy in loads:
        copy.start()
    ready = (
        (grad_gate, out_gate), (grad_up, out_up), (grad_down, out_down),
        (grad_gate_pre, out_gate_pre),
    )
    stores = [pltpu.make_async_copy(a, b, sems.at[2 + i]) for i, (a, b) in enumerate(ready)]
    for copy in stores:
        copy.start()
    bf16 = jnp.bfloat16
    proj_block[...] = contract_rows(pieces[...], mixed_all[...])
    stores.append(pltpu.make_async_copy(proj_block, out_proj, sems.at[6]))
    stores[-1].start()
    grad = state_grad[...]
    d_recur = (grad * recur_part[...]).astype(bf16)
    d_input = (grad * input_part[...]).astype(bf16)
    for copy in loads:
        copy.wait()
    width = recur_map.shape[1]
    for group in range(recur_map.shape[0]):
        columns = slice(group * width, (group + 1) * width)
        through = contract_columns(d_recur[:, columns], recur_map[group])
        through = through + contract_columns(d_input[:, columns], input_map[group])
        conv_block[:, columns] = (
            state_grad[:, columns] * conv_part[:, columns] + through
        ).astype(bf16)
    stores.append(pltpu.make_async_copy(conv_block, out_conv, sems.at[7]))
    stores[-1].start()
    for copy in stores:
        copy.wait()


def run_dense(experts, tps, capacity, maps, *operands):
    row_block, w_gate = operands[0], operands[11]
    tokens, width = row_block.shape
    features = tps * width
    hidden = w_gate.shape[1]
    slots, n_z = experts * capacity, experts // 2
    bf16, f32 = jnp.bfloat16, jnp.float32
    outer = pl.BlockSpec(memory_space=pltpu.HBM)
    tile, wide = (tokens, width), (tokens, features)
    cut = features // experts
    weight, down = (features, hidden), (hidden, features)
    struct = jax.ShapeDtypeStruct
    results = [
        struct((experts, tokens, width), bf16),
        struct((experts, tokens, cut), bf16),
        struct(weight, bf16),
        struct(weight, bf16),
        struct(down, bf16),
        struct(tile, f32),
        struct(tile, f32),
        struct(tile, f32),
        struct(tile, f32),
        struct(tile, bf16),
    ]
    done = pl.pallas_call(
        functools.partial(expert_kernel, experts, tps, capacity),
        out_shape=results,
        in_specs=[outer] * len(operands),
        out_specs=[VMEM] * len(results),
        scratch_shapes=[pltpu.VMEM(operand.shape, operand.dtype) for operand in operands]
        + [
            pltpu.VMEM((2, n_z, *tile), bf16),
            pltpu.VMEM((n_z, 2 * experts, tokens), f32),
            pltpu.VMEM((2, slots, features), bf16),
            pltpu.VMEM((2, n_z, capacity, width), bf16),
            pltpu.VMEM((slots, hidden), bf16),
            pltpu.VMEM((slots, hidden), bf16),
            pltpu.VMEM((slots, hidden), bf16),
            pltpu.VMEM((2, slots, width), bf16),
            pltpu.VMEM((2, slots, width), f32),
            pltpu.VMEM((2, slots, width), bf16),
            pltpu.VMEM((slots, width), bf16),
            pltpu.VMEM((slots, width), bf16),
            pltpu.VMEM((slots, width), bf16),
            pltpu.VMEM((slots, width), bf16),
            pltpu.VMEM((slots, tokens), bf16),
            pltpu.VMEM(wide, bf16),
            pltpu.VMEM(tile, bf16),
            pltpu.VMEM(tile, f32),
            pltpu.VMEM(tile, f32),
            pltpu.VMEM(tile, f32),
            pltpu.VMEM(tile, f32),
            pltpu.VMEM(tile, f32),
            pltpu.VMEM((2, width), f32),
            pltpu.VMEM((experts, 2, width), f32),
            DMA((len(operands),)),
            DMA((2, n_z, 2)),
            DMA((2, n_z)),
            DMA((n_z, 2)),
            DMA((n_z,)),
            DMA((2, n_z)),
            DMA((2, n_z)),
            DMA((2, experts, tps)),
            DMA((2, experts, tps)),
            DMA((n_z, 2)),
            DMA((n_z, 2)),
            DMA((n_z,)),
            DMA((n_z,)),
            DMA((experts,)),
            DMA((experts,)),
            DMA((n_z, 3)),
            DMA((experts,)),
            DMA((tps,)),
            DMA((tps,)),
            DMA((experts, 2)),
            DMA((experts,)),
            DMA((experts,)),
            DMA((2, experts)),
            DMA,
        ],
        compiler_params=pltpu.CompilerParams(
            collective_id=3, has_side_effects=True, vmem_limit_bytes=32 * 1024 * 1024
        ),
    )(*[pltpu.with_memory_space_constraint(each, pltpu.HBM) for each in operands])
    mixed_all, pieces, *others = done
    everything = [
        mixed_all.reshape(experts * tokens, width), pieces.reshape(experts * tokens, cut), *others,
    ]
    finals = [
        struct(weight, bf16),
        struct(weight, bf16),
        struct(down, bf16),
        struct((cut, width), f32),
        struct(tile, bf16),
        struct(tile, bf16),
    ]
    return pl.pallas_call(
        finish_kernel,
        out_shape=finals,
        in_specs=[VMEM] * len(everything) + [outer] * 2,
        out_specs=[outer] * len(finals),
        scratch_shapes=[pltpu.VMEM(each.shape, each.dtype) for each in maps]
        + [pltpu.VMEM((cut, width), f32), pltpu.VMEM(tile, bf16), DMA((8,))],
        compiler_params=pltpu.CompilerParams(vmem_limit_bytes=16 * 1024 * 1024),
    )(*everything, *[pltpu.with_memory_space_constraint(each, pltpu.HBM) for each in maps])


def dispatch_kernel(n_sp, n_tp, rows, cots, got_rows, got_cots, own_sem, sa, ra, st, rt):
    s, t = lax.axis_index("sp"), lax.axis_index("tp")
    width = rows.shape[-1]
    kinds = ((rows, got_rows), (cots, got_cots))
    greet(
        [(flip(s, m), t) for m in range(1, n_sp)] + [(s, flip(t, b)) for b in bits_of(n_tp)]
    )

    def own(kind):
        source, target = kinds[kind]
        return pltpu.make_async_copy(
            source.at[s], target.at[s, :, window(t, width)], own_sem.at[kind]
        )

    def to_expert(kind, m):
        source, target = kinds[kind]
        q = flip(s, m)
        return remote(
            source.at[q], target.at[s, :, window(t, width)], sa.at[kind, m], ra.at[kind, m], (q, t)
        )

    def share(kind, m, k):
        bit = low_bit(k)
        block = kinds[kind][1].at[flip(s, m), :, window(flip(t, k - bit), width)]
        return remote(block, block, st.at[kind, m, k], rt.at[kind, m, k], (s, flip(t, bit)))

    seen = set()

    def forward(m):
        for kind in range(2):
            for k in relays_of(n_tp):
                before = k - low_bit(k)
                if (kind, m, before) not in seen:
                    share(kind, m, before).wait_recv()
                    seen.add((kind, m, before))
                share(kind, m, k).start()

    for kind in range(2):
        own(kind).start()
    for m in range(1, n_sp):
        for kind in range(2):
            to_expert(kind, m).start()
    for m in range(n_sp):
        for kind in range(2):
            if m == 0:
                own(kind).wait()
            else:
                to_expert(kind, m).wait_recv()
            for bit in bits_of(n_tp):
                share(kind, m, bit).start()
        if m > 0:
            forward(m - 1)
    forward(n_sp - 1)
    for kind in range(2):
        for m in range(n_sp):
            if m > 0:
                to_expert(kind, m).wait_send()
            for k in range(1, n_tp):
                share(kind, m, k).wait_send()
                if (kind, m, k) not in seen:
                    share(kind, m, k).wait_recv()


def combine_kernel(
    n_sp, n_tp, part, mixed, base, pick, out, mixed_all, half, xsend, xrecv, back, ret,
    own_sem, sh, rh, sx, rx, sb, rb, sg, rg, st, rt,
):
    s, t = lax.axis_index("sp"), lax.axis_index("tp")
    width = ret.shape[-1]
    pair, across = flip(t, 1), flip(t, 2)
    greet(
        [(flip(s, m), t) for m in range(1, n_sp)] + [(s, flip(t, b)) for b in bits_of(n_tp)]
    )

    def to_pair(slot):
        chunk = flip(pair, 2) if slot == 0 else pair
        return remote(
            part.at[:, :, window(chunk, width)], half.at[slot], sh.at[slot], rh.at[slot], (s, pair)
        )

    def cross(m):
        q = flip(s, m)
        return remote(xsend.at[q], xrecv.at[q], sx.at[m], rx.at[m], (s, across))

    def give(m):
        q = flip(s, m)
        return remote(back.at[q], ret.at[s], sb.at[m], rb.at[m], (q, t))

    def gather(k):
        bit = low_bit(k)
        block = flip(s, k - bit)
        source = mixed if k == bit else mixed_all.at[block]
        return remote(source, mixed_all.at[block], sg.at[k], rg.at[k], (flip(s, bit), t))

    seen = set()

    def forward(masks):
        for k in masks:
            before = k - low_bit(k)
            if before not in seen:
                gather(before).wait_recv()
                seen.add(before)
            gather(k).start()

    to_pair(0).start()
    to_pair(1).start()
    own = pltpu.make_async_copy(mixed, mixed_all.at[s], own_sem)
    own.start()
    for bit in bits_of(n_sp):
        gather(bit).start()
    order = list(range(n_sp - 1, -1, -1))
    to_pair(0).wait_recv()
    for m in order:
        q = flip(s, m)
        xsend[q] = (
            part[q, :, window(across, width)].astype(jnp.float32) + half[0, q].astype(jnp.float32)
        ).astype(jnp.bfloat16)
        cross(m).start()
    to_pair(1).wait_recv()
    relays = relays_of(n_sp)
    early = [k for k in relays if bin(k).count("1") == 2]
    forward(early)
    for place, m in enumerate(order):
        q = flip(s, m)
        cross(m).wait_recv()
        total = (
            part[q, :, window(t, width)].astype(jnp.float32)
            + half[1, q].astype(jnp.float32)
            + xrecv[q].astype(jnp.float32)
        ).astype(jnp.bfloat16)
        if m == 0:
            ret[s] = total
        else:
            back[q] = total
            give(m).start()
        if place == n_sp // 2:
            forward([k for k in relays if k not in early])
    total = base[...].astype(jnp.float32)
    for m in range(n_sp):
        q = flip(s, m)
        if m > 0:
            give(m).wait_recv()
        total = total + contract_rows(pick[q], ret[q])
    out[:, window(t, width)] = total.astype(jnp.bfloat16)

    def share(k):
        bit = low_bit(k)
        block = out.at[:, window(flip(t, k - bit), width)]
        return remote(block, block, st.at[k], rt.at[k], (s, flip(t, bit)))

    for bit in bits_of(n_tp):
        share(bit).start()
    shared = set()
    for k in relays_of(n_tp):
        before = k - low_bit(k)
        if before not in shared:
            share(before).wait_recv()
            shared.add(before)
        share(k).start()
    for k in range(1, n_tp):
        share(k).wait_send()
        if k not in shared:
            share(k).wait_recv()
    own.wait()
    for slot in range(2):
        to_pair(slot).wait_send()
    for m in range(n_sp):
        cross(m).wait_send()
        if m > 0:
            give(m).wait_send()
            gather(m).wait_send()
            if m not in seen:
                gather(m).wait_recv()


def scan_kernel(
    n_sp, flipped, drive, decay, state_grad, pieces, weight, carry, carries,
    own_sem, sa, ra, sc, rc,
):
    s, t = lax.axis_index("sp"), lax.axis_index("tp")
    rows = drive.shape[0]
    share = flipped.shape[0] // n_sp
    greet([(flip(s, m), t) for m in range(1, n_sp)])

    def piece(m):
        q = flip(s, m)
        return remote(
            flipped.at[window(q, share)], pieces.at[:, window(s, rows)], sa.at[m], ra.at[m], (q, t)
        )

    def send_carry(m):
        return remote(carry, carries.at[s], sc.at[m], rc.at[m], (flip(s, m), t))

    own = pltpu.make_async_copy(
        flipped.at[window(s, share)], pieces.at[:, window(s, rows)], own_sem
    )
    own.start()

    def lap(step, held):
        grad, product = held
        row = rows - 1 - step
        grad = drive[pl.ds(row, 1), :] + grad
        product_here = product
        state_grad[pl.ds(row, 1), :] = grad
        weight[pl.ds(row, 1), :] = product_here
        now = decay[pl.ds(row, 1), :]
        return (now * grad, now * product_here)

    zero = jnp.zeros((1, drive.shape[1]), jnp.float32)
    start, span = lax.fori_loop(0, rows, lap, (zero, zero + 1.0), unroll=8)
    carry[0:1, :] = span
    carry[1:2, :] = start
    for m in range(1, n_sp):
        send_carry(m).start()
    for m in range(1, n_sp):
        piece(m).start()
    for m in range(1, n_sp):
        send_carry(m).wait_recv()
    incoming = zero
    for later in range(n_sp - 1, 0, -1):
        longer = carries[later, 1:2, :] + carries[later, 0:1, :] * incoming
        incoming = jnp.where(later > s, longer, incoming)
    state_grad[...] = state_grad[...] + weight[...] * incoming
    own.wait()
    for m in range(1, n_sp):
        send_carry(m).wait_send()
        piece(m).wait_send()
        piece(m).wait_recv()


def silu_parts(values):
    sig = jax.nn.sigmoid(values)
    return (values * sig, sig * (1.0 + values * (1.0 - sig)))


def route_slots(route_block, experts, capacity):
    flat_ids = route_block.reshape(-1)
    onehot = (flat_ids[:, None] == jnp.arange(experts, dtype=jnp.int32)[None, :]).astype(jnp.int32)
    before = jnp.cumsum(onehot, axis=0) - onehot
    slot_rank = jnp.sum(before * onehot, axis=1)
    return flat_ids * capacity + slot_rank


def contract_rows(left, right):
    return lax.dot_general(
        left, right, (((0,), (0,)), ((), ())), preferred_element_type=jnp.float32
    )


def sparse_body(
    cotangent,
    mixer_out,
    route_ids,
    route_weights,
    conv_out,
    recur_gate,
    input_gate,
    gate_pre,
    states_before,
    decay_rate,
    out_proj,
    recur_map,
    input_map,
    expert_gate,
    expert_up,
    expert_down,
):
    row_count = cotangent.shape[0]
    experts = lax.axis_size("sp")
    capacity = 4 * row_count // experts
    slot_pos = route_slots(route_ids, experts, capacity).reshape(row_count, 2)
    slot_range = jnp.arange(experts * capacity, dtype=jnp.int32)[:, None]
    hit_first = slot_range == slot_pos[None, :, 0]
    hit_second = slot_range == slot_pos[None, :, 1]
    dispatch = (hit_first | hit_second).astype(jnp.bfloat16)
    slot_weight = jnp.sum(
        jnp.where(hit_first, route_weights[None, :, 0], 0.0)
        + jnp.where(hit_second, route_weights[None, :, 1], 0.0),
        axis=1,
    )
    send_rows = jnp.dot(dispatch, mixer_out, preferred_element_type=jnp.float32).astype(
        jnp.bfloat16
    )
    send_cot = (
        jnp.dot(dispatch, cotangent, preferred_element_type=jnp.float32) * slot_weight[:, None]
    ).astype(jnp.bfloat16)
    tps = lax.axis_size("tp")
    features = tps * cotangent.shape[1]
    slots = experts * capacity
    blocks = (experts, capacity, features)
    got_rows, got_cot = call(
        functools.partial(dispatch_kernel, experts, tps),
        [jax.ShapeDtypeStruct(blocks, jnp.bfloat16)] * 2,
        [
            DMA((2,)),
            DMA((2, experts)),
            DMA((2, experts)),
            DMA((2, experts, tps)),
            DMA((2, experts, tps)),
        ],
        0,
        send_rows.reshape(experts, capacity, -1),
        send_cot.reshape(experts, capacity, -1),
    )
    got_rows, got_cot = (got_rows.reshape(slots, features), got_cot.reshape(slots, features))
    w_gate = expert_gate[0]
    w_up = expert_up[0]
    w_down = expert_down[0]
    pre_gate = jnp.dot(got_rows, w_gate, preferred_element_type=jnp.float32)
    pre_up = jnp.dot(got_rows, w_up, preferred_element_type=jnp.float32)
    gate_act, slope = silu_parts(pre_gate)
    active = (gate_act * pre_up).astype(jnp.bfloat16)
    d_active = lax.dot_general(
        got_cot, w_down, (((1,), (1,)), ((), ())), preferred_element_type=jnp.float32
    )
    grad_down = contract_rows(active, got_cot).astype(jnp.bfloat16)
    d_gate = (d_active * pre_up * slope).astype(jnp.bfloat16)
    d_up = (d_active * gate_act).astype(jnp.bfloat16)
    grad_gate = contract_rows(got_rows, d_gate).astype(jnp.bfloat16)
    grad_up = contract_rows(got_rows, d_up).astype(jnp.bfloat16)
    partial_grad = lax.dot_general(
        d_gate, w_gate, (((1,), (1,)), ((), ())), preferred_element_type=jnp.float32
    ) + lax.dot_general(d_up, w_up, (((1,), (1,)), ((), ())), preferred_element_type=jnp.float32)
    channels = conv_out.shape[1]
    rate = decay_rate[None, :]
    recur_f = recur_gate.astype(jnp.float32)
    input_f = input_gate.astype(jnp.float32)
    conv_f = conv_out.astype(jnp.float32)
    before_f = states_before.astype(jnp.float32)
    log_decay = -8.0 * recur_f * rate
    decay_now = jnp.exp(log_decay)
    position = lax.axis_index("sp") * row_count + jnp.arange(row_count, dtype=jnp.int32)
    at_start = (position == 0)[:, None]
    norm_factor = jnp.where(at_start, 1.0, jnp.sqrt(-jnp.expm1(2.0 * log_decay)))
    norm_slope = jnp.where(at_start, 0.0, -jnp.exp(2.0 * log_decay) / norm_factor)
    drive = input_f * conv_f
    state = decay_now * before_f + norm_factor * drive
    gate, gelu_back = jax.vjp(jax.nn.gelu, gate_pre.astype(jnp.float32))
    mixed = (state * gate).astype(jnp.bfloat16)
    block = (experts, capacity, cotangent.shape[1])
    pair_sems, own_sems = (DMA((2,)), DMA((experts,)))
    tp_sems = DMA((tps,))
    out_grad, mixed_all = call(
        functools.partial(combine_kernel, experts, tps),
        [
            jax.ShapeDtypeStruct((row_count, features), jnp.bfloat16),
            jax.ShapeDtypeStruct((experts, row_count, channels), jnp.bfloat16),
        ],
        [
            pltpu.VMEM((2, *block), jnp.bfloat16),
            pltpu.VMEM(block, jnp.bfloat16),
            pltpu.VMEM(block, jnp.bfloat16),
            pltpu.VMEM(block, jnp.bfloat16),
            pltpu.VMEM(block, jnp.bfloat16),
            DMA,
            pair_sems,
            pair_sems,
            *([own_sems] * 6),
            tp_sems,
            tp_sems,
        ],
        1,
        partial_grad.astype(jnp.bfloat16).reshape(blocks),
        mixed,
        cotangent,
        dispatch.reshape(experts, capacity, row_count),
    )
    d_mixed = jnp.dot(out_grad, out_proj, preferred_element_type=jnp.float32)
    state_grad, pieces = call(
        functools.partial(scan_kernel, experts),
        [
            jax.ShapeDtypeStruct((row_count, channels), jnp.float32),
            jax.ShapeDtypeStruct((features // experts, experts * row_count), jnp.bfloat16),
        ],
        [
            pltpu.VMEM((row_count, channels), jnp.float32),
            pltpu.VMEM((2, channels), jnp.float32),
            pltpu.VMEM((experts, 2, channels), jnp.float32),
            DMA,
            *([own_sems] * 4),
        ],
        2,
        out_grad.T,
        d_mixed * gate,
        decay_now,
    )
    grad_out_proj = jnp.dot(
        pieces,
        mixed_all.reshape(experts * row_count, channels),
        preferred_element_type=jnp.float32,
    )
    grad_gate_pre = gelu_back(d_mixed * state)[0].astype(jnp.bfloat16)
    d_log = state_grad * (decay_now * before_f + norm_slope * drive)
    d_recur_pre = (d_log * (-8.0 * rate) * recur_f * (1.0 - recur_f)).astype(jnp.bfloat16)
    d_input_pre = (state_grad * norm_factor * conv_f * input_f * (1.0 - input_f)).astype(
        jnp.bfloat16
    )
    groups = recur_map.shape[0]
    width = recur_map.shape[1]
    through_recur = jnp.einsum(
        "tbj,bij->tbi",
        d_recur_pre.reshape(row_count, groups, width),
        recur_map,
        preferred_element_type=jnp.float32,
    )
    through_input = jnp.einsum(
        "tbj,bij->tbi",
        d_input_pre.reshape(row_count, groups, width),
        input_map,
        preferred_element_type=jnp.float32,
    )
    grad_conv = (
        state_grad * norm_factor * input_f
        + (through_recur + through_input).reshape(row_count, channels)
    ).astype(jnp.bfloat16)
    return (
        grad_gate[None],
        grad_up[None],
        grad_down[None],
        grad_out_proj,
        grad_conv,
        grad_gate_pre,
    )


def body(
    cotangent,
    mixer_out,
    route_ids,
    route_weights,
    conv_out,
    recur_gate,
    input_gate,
    gate_pre,
    states_before,
    decay_rate,
    out_proj,
    recur_map,
    input_map,
    expert_gate,
    expert_up,
    expert_down,
):
    experts, tps = lax.axis_size("sp"), lax.axis_size("tp")
    row_count = cotangent.shape[0]
    capacity = 4 * row_count // experts
    if 2 * capacity < row_count:
        return sparse_body(
            cotangent,
            mixer_out,
            route_ids,
            route_weights,
            conv_out,
            recur_gate,
            input_gate,
            gate_pre,
            states_before,
            decay_rate,
            out_proj,
            recur_map,
            input_map,
            expert_gate,
            expert_up,
            expert_down,
        )
    grad_gate, grad_up, grad_down, grad_out_proj, grad_conv, grad_gate_pre = run_dense(
        experts,
        tps,
        capacity,
        (recur_map, input_map),
        mixer_out,
        cotangent,
        route_ids.T,
        route_weights.T,
        conv_out,
        recur_gate,
        input_gate,
        gate_pre,
        states_before,
        decay_rate[None, :],
        out_proj,
        expert_gate[0],
        expert_up[0],
        expert_down[0],
    )
    return (
        grad_gate[None],
        grad_up[None],
        grad_down[None],
        grad_out_proj,
        grad_conv,
        grad_gate_pre,
    )


def solution(mesh):
    placed = (
        P("sp", "tp"),
        P("sp", "tp"),
        P("sp", None),
        P("sp", None),
        P("sp", "tp"),
        P("sp", "tp"),
        P("sp", "tp"),
        P("sp", "tp"),
        P("sp", "tp"),
        P("tp"),
        P(None, "tp"),
        P("tp", None, None),
        P("tp", None, None),
        P("sp", None, "tp"),
        P("sp", None, "tp"),
        P("sp", "tp", None),
    )
    return jax.shard_map(
        body,
        mesh=mesh,
        in_specs=placed,
        out_specs=(
            P("sp", None, "tp"),
            P("sp", None, "tp"),
            P("sp", "tp", None),
            P("sp", "tp"),
            P("sp", "tp"),
            P("sp", "tp"),
        ),
        check_vma=False,
    )
```

```python
import functools

import jax
import jax.numpy as jnp
from jax import lax
from jax.experimental import pallas as pl
from jax.experimental.pallas import tpu as pltpu
from jax.sharding import PartitionSpec as P

MESH = pl.DeviceIdType.MESH
VMEM = pl.BlockSpec(memory_space=pltpu.VMEM)
DMA = pltpu.SemaphoreType.DMA


def bits_of(count):
    found, bit = [], 1
    while bit < count:
        found.insert(0, bit)
        bit *= 2
    return found


def low_bit(mask):
    return mask & -mask


def flip(index, mask):
    bit = 1
    while bit <= mask:
        if mask & bit:
            index = index + bit - 2 * bit * lax.rem(lax.div(index, bit), 2)
        bit *= 2
    return index


def window(index, width):
    return pl.ds(pl.multiple_of(index * width, width), width)


def remote(source, target, send_sem, recv_sem, device):
    return pltpu.make_async_remote_copy(
        src_ref=source,
        dst_ref=target,
        send_sem=send_sem,
        recv_sem=recv_sem,
        device_id=device,
        device_id_type=MESH,
    )


def greet(peers):
    barrier = pltpu.get_barrier_semaphore()
    for peer in peers:
        pl.semaphore_signal(barrier, inc=1, device_id=peer, device_id_type=MESH)
    pl.semaphore_wait(barrier, len(peers))


def relays_of(count):
    masks = [mask for mask in range(1, count) if mask != low_bit(mask)]
    return sorted(masks, key=lambda mask: (bin(mask).count("1"), -mask))


def call(kernel, out_shape, scratch, ident, *operands):
    return pl.pallas_call(
        kernel,
        out_shape=out_shape,
        in_specs=[VMEM] * len(operands),
        out_specs=jax.tree.map(lambda _: VMEM, out_shape),
        scratch_shapes=scratch,
        compiler_params=pltpu.CompilerParams(
            collective_id=ident, has_side_effects=True, vmem_limit_bytes=48 * 1024 * 1024
        ),
    )(*operands)


def along(index, table):
    found = 0
    for place, value in enumerate(table):
        found = found + jnp.where(index == place, value, 0)
    return found


def abs_of(value):
    return jnp.where(value < 0, -value, value)


def nearest(count):
    return [sorted(range(count), key=lambda other: (abs(other - z), other)) for z in range(count)]


def contract_columns(left, right):
    return lax.dot_general(
        left, right, (((1,), (1,)), ((), ())), preferred_element_type=jnp.float32
    )


def expm1_of(values):
    near = 1.0 / 362880.0
    for factor in (40320.0, 5040.0, 720.0, 120.0, 24.0, 6.0, 2.0, 1.0):
        near = near * values + 1.0 / factor
    return jnp.where(jnp.abs(values) < 0.3, values * near, jnp.exp(values) - 1.0)


def expert_kernel(
    n_sp, n_tp, capacity,
    rows_hbm, cots_hbm, ids_hbm, weights_hbm, conv_hbm, recur_hbm, input_hbm, gate_hbm,
    before_hbm, rate_hbm, proj_hbm, w_gate_hbm, w_up_hbm, w_down_hbm, recur_map_hbm,
    input_map_hbm,
    proj_block, grad_gate, grad_up, grad_down, grad_conv, grad_gate_pre,
    rows, cots, ids, weights, conv, recur, inputs, gate_pre, before, rate, proj,
    w_gate, w_up, w_down, recur_map, input_map,
    tok, meta, got, ybuf, act, dgate, dup, give_pair, mine, half,
    xsend, xrecv, back, ret, pick, mixed_all, pieces, out, mixed, decay, gate, gate_part, drive, product,
    state_grad, recur_part, input_part, conv_part, carry, carries,
    lsem, tss, trs, mss, mrs, yss, yrs, hss, hrs, hds, pss, prs, css, crs, gss, grs,
    zss, zrs, oss, ors, iss, irs, kss, krs, own_sem,
):
    s, t = lax.axis_index("sp"), lax.axis_index("tp")
    n_y = 2
    n_z = n_sp // n_y
    z, y = lax.div(s, n_y), lax.rem(s, n_y)
    beside = flip(s, 1)
    pair, across = flip(t, 1), flip(t, 2)
    tokens, width = rows.shape
    chunk = n_y * capacity
    f32, bf16 = jnp.float32, jnp.bfloat16
    order = [along(z, [found[k] for found in nearest(n_z)]) for k in range(n_z)]

    fetch = [
        pltpu.make_async_copy(source, target, lsem.at[i])
        for i, (source, target) in enumerate(
            (
                (rows_hbm, rows), (cots_hbm, cots), (ids_hbm, ids), (weights_hbm, weights),
                (conv_hbm, conv), (recur_hbm, recur), (input_hbm, inputs), (gate_hbm, gate_pre),
                (before_hbm, before), (rate_hbm, rate),
                (w_gate_hbm, w_gate), (w_up_hbm, w_up), (w_down_hbm, w_down), (proj_hbm, proj),
                (recur_map_hbm, recur_map), (input_map_hbm, input_map),
            )
        )
    ]
    for copy in fetch:
        copy.start()
    barrier_peers = [(flip(s, m), t) for m in range(1, n_sp)]
    barrier_peers += [(flip(s, m), flip(t, 2)) for m in range(1, n_sp)]
    greet(barrier_peers + [(s, flip(t, b)) for b in bits_of(n_tp)])
    for copy in fetch[:4]:
        copy.wait()
    ends = []

    def begin(copy, valid=None, alone=True):
        if alone:
            ends.append((copy, valid))
        if valid is None:
            copy.start()
        else:
            pl.when(valid)(copy.start)

    def spread(make, zb, first):
        above, below = z + 1 < n_z, z >= 1
        if not first:
            above, below = (zb < z) & above, (zb > z) & below
        begin(make(zb, z + 1, 0), above)
        begin(make(zb, z - 1, 1), below)

    def along_line(source, target, send_sem, recv_sem, z_to):
        return remote(source, target, send_sem, recv_sem, (z_to * n_y + y, t))

    def move_tokens(kind, zb, z_to, way, own):
        target = tok.at[kind, zb]
        source = (rows, cots)[kind] if own else target
        return along_line(source, target, tss.at[kind, zb, way], trs.at[kind, zb], z_to)

    def move_meta(zb, z_to, way):
        return along_line(meta.at[zb], meta.at[zb], mss.at[zb, way], mrs.at[zb], z_to)

    def move_mixed(zb, z_to, way, own):
        target = mixed_all.at[zb * n_y + y]
        source = mixed if own else target
        return along_line(source, target, zss.at[zb, way], zrs.at[zb * n_y + y], z_to)

    def mixed_beside(zb, own):
        target = mixed_all.at[zb * n_y + y]
        source = mixed if own else target
        return remote(source, target, zss.at[zb, 2], zrs.at[zb * n_y + y], (beside, t))

    def mixed_from_beside(zb):
        target = mixed_all.at[zb * n_y + 1 - y]
        return remote(mixed, target, zss.at[zb, 2], zrs.at[zb * n_y + 1 - y], (beside, t))

    def slots(kind, block, quarter):
        return got.at[kind, window(block, capacity), window(quarter, width)]

    def to_beside(kind, zb):
        return remote(
            ybuf.at[kind, zb], slots(kind, zb * n_y + y, t),
            yss, yrs.at[kind, zb], (beside, t),
        )

    def from_beside(kind, zb):
        return remote(
            ybuf.at[kind, zb], slots(kind, zb * n_y + 1 - y, t),
            yss, yrs.at[kind, zb], (beside, t),
        )

    def share(kind, block, k):
        bit = low_bit(k)
        ref = slots(kind, block, flip(t, k - bit))
        recv_sem = hrs.at[kind, block] if k == 2 else hds.at[lax.div(block, n_y)]
        return remote(ref, ref, hss, recv_sem, (s, flip(t, bit)))

    def crossed(kind, block):
        ref = slots(kind, block, across)
        return remote(ref, ref, hss, hrs.at[kind, block], (s, across))

    table_rows = lax.broadcasted_iota(jnp.int32, (2 * n_sp, tokens), 0)
    first_id, second_id = ids[0:1, :], ids[1:2, :]
    hits = ((first_id == table_rows) | (second_id == table_rows)).astype(f32)
    earlier = lax.broadcasted_iota(jnp.int32, (tokens, tokens), 0) < lax.broadcasted_iota(
        jnp.int32, (tokens, tokens), 1
    )
    rank = jnp.dot(
        hits.astype(bf16), earlier.astype(f32).astype(bf16), preferred_element_type=f32
    )
    rank = jnp.where(hits > 0.0, rank, -1.0)
    weight_rows = table_rows - n_sp
    weight = jnp.where(first_id == weight_rows, weights[0:1, :], 0.0) + jnp.where(
        second_id == weight_rows, weights[1:2, :], 0.0
    )
    meta[z] = jnp.where(table_rows < n_sp, rank, weight)

    spread(lambda zb, to, way: move_tokens(0, zb, to, way, True), z, True)
    spread(move_meta, z, True)
    spread(lambda zb, to, way: move_tokens(1, zb, to, way, True), z, True)

    slot_index = lax.broadcasted_iota(jnp.int32, (capacity, tokens), 0).astype(f32)

    def chosen(zb, expert):
        return meta[zb, pl.ds(expert, 1), :] == slot_index

    def compact(kind, k, valid=None):
        zb = order[k]
        block = zb * n_y + y
        sends = (to_beside(kind, zb), share(kind, block, 2), share(kind, block, 1))

        def work():
            picks = jnp.concatenate(
                [chosen(zb, s).astype(f32), chosen(zb, beside).astype(f32)], axis=0
            )
            source = tok[kind, zb] if k > 0 else (rows, cots)[kind][...]
            found = jnp.dot(picks.astype(bf16), source, preferred_element_type=f32)
            if kind == 1:
                table = jnp.concatenate(
                    [
                        jnp.broadcast_to(meta[zb, pl.ds(n_sp + e, 1), :], (capacity, tokens))
                        for e in (s, beside)
                    ],
                    axis=0,
                )
                found = found * jnp.sum(picks * table, axis=1, keepdims=True)
            found = found.astype(bf16)
            ybuf[kind, zb] = found[capacity:]
            got[kind, window(block, capacity), window(t, width)] = found[:capacity]
            for copy in sends:
                copy.start()

        if valid is None:
            work()
        else:
            pl.when(valid)(work)

    def hear(distance, kind):
        for k in range(1, n_z):
            apart = {abs(found[k] - place) for place, found in enumerate(nearest(n_z))}
            if distance not in apart:
                continue
            zb = order[k]
            only = None if len(apart) == 1 else abs_of(zb - z) == distance
            waits = [move_tokens(kind, zb, z, 0, False)] + [move_meta(zb, z, 0)] * (kind == 0)
            for copy in waits:
                if only is None:
                    copy.wait_recv()
                else:
                    pl.when(only)(copy.wait_recv)
            make = [lambda zb, to, way: move_tokens(kind, zb, to, way, False)]
            for made in make + [move_meta] * (kind == 0):
                above, below = (zb < z) & (z + 1 < n_z), (zb > z) & (z >= 1)
                if only is not None:
                    above, below = above & only, below & only
                begin(made(zb, z + 1, 0), above)
                begin(made(zb, z - 1, 1), below)
        for k in range(1, n_z):
            apart = {abs(found[k] - place) for place, found in enumerate(nearest(n_z))}
            if distance in apart:
                only = None if len(apart) == 1 else abs_of(order[k] - z) == distance
                compact(kind, k, only)

    def take_beside(kind, k):
        block = order[k] * n_y + 1 - y
        from_beside(kind, order[k]).wait_recv()
        begin(share(kind, block, 2), alone=False)
        begin(share(kind, block, 1), alone=False)

    def relay_x(kind, k):
        for block in (order[k] * n_y + y, order[k] * n_y + 1 - y):
            crossed(kind, block).wait_recv()
            begin(share(kind, block, 3), alone=False)

    def gather_chunk(k):
        both = got.at[:, window(order[k], chunk), pl.ds(0, (n_tp // 2) * width)]
        remote(both, both, hss, hds.at[order[k]], (s, pair)).wait_recv()

    def to_pair(zb, slot):
        here = window(zb, chunk)
        return remote(
            give_pair.at[slot, here], half.at[slot, here],
            pss, prs.at[zb, slot], (s, pair),
        )

    def cross(zb):
        here = window(zb, chunk)
        return remote(xsend.at[here], xrecv.at[here], css, crs.at[zb], (s, across))

    def give(block):
        here = window(block, capacity)
        return remote(
            back.at[here], ret.at[window(s, capacity)], gss, grs, (block, t)
        )

    def given():
        most = pl.ds(0, (n_sp - 1) * capacity)
        return remote(back.at[most], ret.at[most], gss, grs, (beside, t))

    def experts(k):
        zb = order[k]
        here = window(zb, chunk)
        got_rows = got[0, here, :]
        pre_gate = jnp.dot(got_rows, w_gate[...], preferred_element_type=f32)
        pre_up = jnp.dot(got_rows, w_up[...], preferred_element_type=f32)
        d_active = contract_columns(got[1, here, :], w_down[...])
        gate_act, slope = silu_parts(pre_gate)
        act[here, :] = (gate_act * pre_up).astype(bf16)
        d_gate = (d_active * pre_up * slope).astype(bf16)
        d_up = (d_active * gate_act).astype(bf16)
        dgate[here, :] = d_gate
        dup[here, :] = d_up

        def partial(quarter):
            columns = window(quarter, width)
            return contract_columns(d_gate, w_gate[columns, :]) + contract_columns(
                d_up, w_up[columns, :]
            )

        give_pair[0, here, :] = partial(flip(pair, 2)).astype(bf16)
        begin(to_pair(zb, 0), alone=False)
        give_pair[1, here, :] = partial(pair).astype(bf16)
        begin(to_pair(zb, 1), alone=False)
        mine[0, here, :] = partial(across)
        mine[1, here, :] = partial(t)

    def send_across(k):
        zb = order[k]
        here = window(zb, chunk)
        to_pair(zb, 0).wait_recv()
        xsend[here, :] = (mine[0, here, :] + half[0, here, :].astype(f32)).astype(bf16)
        begin(cross(zb), alone=False)

    def send_home(k):
        zb = order[k]
        here = window(zb, chunk)
        to_pair(zb, 1).wait_recv()
        cross(zb).wait_recv()
        total = (
            mine[1, here, :] + half[1, here, :].astype(f32) + xrecv[here, :].astype(f32)
        ).astype(bf16)
        back[here, :] = total
        if k > 0:
            begin(give(zb * n_y + y), alone=False)
        else:
            ret[window(s, capacity), :] = back[window(s, capacity), :]
        begin(give(zb * n_y + 1 - y), alone=False)

    step = 256 if width % 256 == 0 else width

    def weight_grad(target, kind, right):
        def lap(j, _):
            columns = window(j, step)
            target[columns, :] = contract_rows(got[kind, :, columns], right[...]).astype(bf16)
            return 0

        lax.fori_loop(0, n_tp * width // step, lap, 0)

    def down_grad():
        def lap(j, _):
            columns = window(j, step)
            grad_down[:, columns] = contract_rows(act[...], got[1, :, columns]).astype(bf16)
            return 0

        lax.fori_loop(0, n_tp * width // step, lap, 0)

    def send_mixed():
        spread(lambda zb, to, way: move_mixed(zb, to, way, True), z, True)
        begin(mixed_beside(z, True))

    def take_mixed(distance):
        for k in range(1, n_z):
            apart = {abs(found[k] - place) for place, found in enumerate(nearest(n_z))}
            if distance not in apart:
                continue
            zb = order[k]
            only = None if len(apart) == 1 else abs_of(zb - z) == distance
            wait = move_mixed(zb, z, 0, False).wait_recv
            if only is None:
                wait()
            else:
                pl.when(only)(wait)
            above, below = (zb < z) & (z + 1 < n_z), (zb > z) & (z >= 1)
            if only is not None:
                above, below = above & only, below & only
            begin(move_mixed(zb, z + 1, 0, False), above)
            begin(move_mixed(zb, z - 1, 1, False), below)
            begin(mixed_beside(zb, False), only)

    def share_out(k):
        bit = low_bit(k)
        ref = out.at[:, window(flip(t, k - bit), width)]
        return remote(ref, ref, oss, ors.at[k - 1], (s, flip(t, bit)))

    def out_arrived(k):
        ref = out.at[:, window(flip(t, k), width)]
        return remote(ref, ref, oss, ors.at[k - 1], (s, flip(t, low_bit(k))))

    strip = 16

    def recurrence():
        def lap(j, _):
            here = window(j, strip)
            rate_row = rate[...]
            recur_f = recur[here, :].astype(f32)
            input_f = inputs[here, :].astype(f32)
            conv_f = conv[here, :].astype(f32)
            before_f = before[here, :].astype(f32)
            gate_f = gate_pre[here, :].astype(f32)
            log_decay = -8.0 * recur_f * rate_row
            decay_now = jnp.exp(log_decay)
            place = lax.broadcasted_iota(jnp.int32, conv_f.shape, 0) + (s * tokens + j * strip)
            at_start = place == 0
            norm = jnp.where(at_start, 1.0, jnp.sqrt(-expm1_of(2.0 * log_decay)))
            slope = jnp.where(at_start, 0.0, -jnp.exp(2.0 * log_decay) / norm)
            entry = input_f * conv_f
            kept = decay_now * before_f
            state = kept + norm * entry
            inner = 0.7978845608028654 * (gate_f + 0.044715 * gate_f * gate_f * gate_f)
            bend = jnp.tanh(inner)
            half_up = 0.5 * (1.0 + bend)
            gate_now = gate_f * half_up
            gate_slope = half_up + 0.5 * gate_f * (1.0 - bend * bend) * 0.7978845608028654 * (
                1.0 + 3.0 * 0.044715 * gate_f * gate_f
            )
            decay[here, :] = decay_now
            gate[here, :] = gate_now
            gate_part[here, :] = state * gate_slope
            mixed[here, :] = (state * gate_now).astype(bf16)
            recur_part[here, :] = (
                (kept + slope * entry) * (-8.0 * rate_row) * recur_f * (1.0 - recur_f)
            )
            input_part[here, :] = norm * conv_f * input_f * (1.0 - input_f)
            conv_part[here, :] = norm * input_f
            return 0

        lax.fori_loop(0, tokens // strip, lap, 0)

        def back_lap(step, held):
            row = tokens - 1 - step
            product[pl.ds(row, 1), :] = held
            return held * decay[pl.ds(row, 1), :]

        one = jnp.ones((1, width), f32)
        carry[0:1, :] = lax.fori_loop(0, tokens, back_lap, one, unroll=8)

    cut = n_tp * width // n_sp
    held_blocks = width // cut

    def piece(j, way):
        q = t * held_blocks + j
        return remote(
            out.at[:, window(q, cut)], pieces.at[s], iss.at[j, way], irs.at[s],
            (q, across if way else t),
        )

    def piece_beside(block):
        return remote(
            pieces.at[block], pieces.at[block], kss, irs.at[block], (s, pair)
        )

    def send_carry(m):
        return remote(carry, carries.at[s], krs.at[0, m], krs.at[1, m], (flip(s, m), t))

    for kind in range(2):
        compact(kind, 0)
    for expert in range(n_sp):
        pick[expert * capacity : (expert + 1) * capacity, :] = (
            chosen(z, expert).astype(f32).astype(bf16)
        )
    for kind in range(2):
        take_beside(kind, 0)
    hear(1, 0)
    hear(1, 1)
    take_beside(0, 1)
    for copy in fetch[4:]:
        copy.wait()
    recurrence()
    own_mixed = pltpu.make_async_copy(mixed, mixed_all.at[s], own_sem)
    own_mixed.start()
    relay_x(0, 0)
    relay_x(1, 0)
    for distance in range(2, n_z):
        hear(distance, 0)
        take_beside(1, distance - 1)
        hear(distance, 1)
        if distance == n_z - 2:
            send_mixed()
        gather_chunk(distance - 2)
        experts(distance - 2)
        take_beside(0, distance)
        for kind in range(2):
            relay_x(kind, distance - 1)
    take_beside(1, n_z - 1)
    send_across(0)
    for k in range(n_z - 2, n_z):
        gather_chunk(k)
        experts(k)
        if k == n_z - 2:
            for kind in range(2):
                relay_x(kind, n_z - 1)
            take_mixed(1)
        send_across(k)
    for distance in range(2, n_z - 1):
        take_mixed(distance)
    send_home(n_z - 2)
    for k in range(1, n_z - 2):
        send_across(k)
    send_home(0)
    down_grad()
    send_home(n_z - 1)
    weight_grad(grad_gate, 0, dgate)
    for k in range(1, n_z - 2):
        send_home(k)
    weight_grad(grad_up, 0, dup)
    take_mixed(n_z - 1)
    given().wait_recv()
    total = cots[...].astype(f32) + contract_rows(pick[...], ret[...])
    out[:, window(t, width)] = total.astype(bf16)
    begin(share_out(2), alone=False)
    begin(share_out(1), alone=False)
    for j in range(held_blocks):
        q = t * held_blocks + j
        begin(piece(j, 0), abs_of(q - s) > 0)
        begin(piece(j, 1), abs_of(q - s) > 0)

    def through_proj(k):
        columns = window(flip(t, k), width)
        return jnp.dot(out[:, columns], proj[columns, :], preferred_element_type=f32)

    drive[...] = through_proj(0)
    out_arrived(1).wait_recv()
    drive[...] += through_proj(1)
    out_arrived(2).wait_recv()
    begin(share_out(3), alone=False)
    drive[...] += through_proj(2)
    out_arrived(3).wait_recv()
    d_mixed = drive[...] + through_proj(3)
    grad_gate_pre[...] = (d_mixed * gate_part[...]).astype(bf16)
    drive[...] = d_mixed * gate[...]

    def lap(step, held):
        row = tokens - 1 - step
        grad = drive[pl.ds(row, 1), :] + held
        state_grad[pl.ds(row, 1), :] = grad
        return decay[pl.ds(row, 1), :] * grad

    zero = jnp.zeros((1, width), f32)
    carry[1:2, :] = lax.fori_loop(0, tokens, lap, zero, unroll=8)
    direct = lax.rem(lax.div(s, held_blocks), 2) == lax.rem(t, 2)
    for m in range(1, n_sp):
        begin(send_carry(m), flip(s, m) < s)
    pieces[s] = out[:, window(s, cut)]
    for m in range(1, n_sp):
        block = flip(s, m)
        pl.when(direct)(piece_beside(block).wait_recv)
        begin(piece_beside(block), direct, alone=False)
    for k in range(n_z):
        mixed_from_beside(order[k]).wait_recv()
    own_mixed.wait()
    for m in range(1, n_sp):
        pl.when(jnp.logical_not(direct))(piece_beside(flip(s, m)).wait_recv)
    proj_block[...] = contract_rows(
        pieces[...].reshape(n_sp * tokens, cut), mixed_all[...].reshape(n_sp * tokens, width)
    )
    for m in range(1, n_sp):
        pl.when(flip(s, m) > s)(send_carry(m).wait_recv)
    incoming = zero
    for later in range(n_sp - 1, 0, -1):
        longer = carries[later, 1:2, :] + carries[later, 0:1, :] * incoming
        incoming = jnp.where(later > s, longer, incoming)
    grad = state_grad[...] + product[...] * incoming
    d_recur = (grad * recur_part[...]).astype(bf16)
    d_input = (grad * input_part[...]).astype(bf16)
    straight = grad * conv_part[...]
    side = recur_map.shape[1]
    for group in range(recur_map.shape[0]):
        columns = slice(group * side, (group + 1) * side)
        through = contract_columns(d_recur[:, columns], recur_map[group])
        through = through + contract_columns(d_input[:, columns], input_map[group])
        grad_conv[:, columns] = (straight[:, columns] + through).astype(bf16)
    some = got.at[:, pl.ds(0, (n_tp - 1) * chunk), :]
    remote(some, some, hss, hds.at[0], (s, pair)).wait_send()
    remote(ybuf, ybuf, yss, yrs.at[0, 0], (beside, t)).wait_send()
    remote(give_pair, half, pss, prs.at[0, 0], (s, pair)).wait_send()
    remote(xsend, xrecv, css, crs.at[0], (s, across)).wait_send()
    given().wait_send()
    others = out.at[:, pl.ds(0, (n_tp - 1) * width)]
    remote(others, others, oss, ors.at[0], (s, pair)).wait_send()
    spare = pieces.at[pl.ds(0, n_sp - 1)]
    pl.when(direct)(remote(spare, spare, kss, irs.at[0], (s, pair)).wait_send)
    for copy, valid in ends:
        if valid is None:
            copy.wait_send()
        else:
            pl.when(valid)(copy.wait_send)


def finish_kernel(*refs):
    count = len(refs) // 2
    sems = refs[-1]
    stores = [
        pltpu.make_async_copy(refs[i], refs[count + i], sems.at[i]) for i in range(count)
    ]
    for copy in stores:
        copy.start()
    for copy in stores:
        copy.wait()


def run_dense(experts, tps, capacity, *operands):
    row_block, w_gate = operands[0], operands[11]
    tokens, width = row_block.shape
    features = tps * width
    hidden = w_gate.shape[1]
    slots, n_z = experts * capacity, experts // 2
    bf16, f32 = jnp.bfloat16, jnp.float32
    outer = pl.BlockSpec(memory_space=pltpu.HBM)
    tile, wide = (tokens, width), (tokens, features)
    cut = features // experts
    weight, down = (features, hidden), (hidden, features)
    struct = jax.ShapeDtypeStruct
    results = [
        struct((cut, width), f32),
        struct(weight, bf16),
        struct(weight, bf16),
        struct(down, bf16),
        struct(tile, bf16),
        struct(tile, bf16),
    ]
    done = pl.pallas_call(
        functools.partial(expert_kernel, experts, tps, capacity),
        out_shape=results,
        in_specs=[outer] * len(operands),
        out_specs=[VMEM] * len(results),
        scratch_shapes=[pltpu.VMEM(operand.shape, operand.dtype) for operand in operands]
        + [
            pltpu.VMEM((2, n_z, *tile), bf16),
            pltpu.VMEM((n_z, 2 * experts, tokens), f32),
            pltpu.VMEM((2, slots, features), bf16),
            pltpu.VMEM((2, n_z, capacity, width), bf16),
            pltpu.VMEM((slots, hidden), bf16),
            pltpu.VMEM((slots, hidden), bf16),
            pltpu.VMEM((slots, hidden), bf16),
            pltpu.VMEM((2, slots, width), bf16),
            pltpu.VMEM((2, slots, width), f32),
            pltpu.VMEM((2, slots, width), bf16),
            pltpu.VMEM((slots, width), bf16),
            pltpu.VMEM((slots, width), bf16),
            pltpu.VMEM((slots, width), bf16),
            pltpu.VMEM((slots, width), bf16),
            pltpu.VMEM((slots, tokens), bf16),
            pltpu.VMEM((experts, tokens, width), bf16),
            pltpu.VMEM((experts, tokens, cut), bf16),
            pltpu.VMEM(wide, bf16),
            pltpu.VMEM(tile, bf16),
            pltpu.VMEM(tile, f32),
            pltpu.VMEM(tile, f32),
            pltpu.VMEM(tile, f32),
            pltpu.VMEM(tile, f32),
            pltpu.VMEM(tile, f32),
            pltpu.VMEM(tile, f32),
            pltpu.VMEM(tile, f32),
            pltpu.VMEM(tile, f32),
            pltpu.VMEM(tile, f32),
            pltpu.VMEM((2, width), f32),
            pltpu.VMEM((experts, 2, width), f32),
            DMA((len(operands),)),
            DMA((2, n_z, 2)),
            DMA((2, n_z)),
            DMA((n_z, 2)),
            DMA((n_z,)),
            DMA,
            DMA((2, n_z)),
            DMA,
            DMA((2, experts)),
            DMA((n_z,)),
            DMA,
            DMA((n_z, 2)),
            DMA,
            DMA((n_z,)),
            DMA,
            DMA,
            DMA((n_z, 3)),
            DMA((experts,)),
            DMA,
            DMA((tps - 1,)),
            DMA((experts // tps, 2)),
            DMA((experts,)),
            DMA,
            DMA((2, experts)),
            DMA,
        ],
        compiler_params=pltpu.CompilerParams(
            collective_id=3, has_side_effects=True, vmem_limit_bytes=32 * 1024 * 1024
        ),
    )(*[pltpu.with_memory_space_constraint(each, pltpu.HBM) for each in operands])
    return pl.pallas_call(
        finish_kernel,
        out_shape=results,
        in_specs=[VMEM] * len(results),
        out_specs=[outer] * len(results),
        scratch_shapes=[DMA((len(results),))],
        compiler_params=pltpu.CompilerParams(vmem_limit_bytes=16 * 1024 * 1024),
    )(*done)


def dispatch_kernel(n_sp, n_tp, rows, cots, got_rows, got_cots, own_sem, sa, ra, st, rt):
    s, t = lax.axis_index("sp"), lax.axis_index("tp")
    width = rows.shape[-1]
    kinds = ((rows, got_rows), (cots, got_cots))
    greet(
        [(flip(s, m), t) for m in range(1, n_sp)] + [(s, flip(t, b)) for b in bits_of(n_tp)]
    )

    def own(kind):
        source, target = kinds[kind]
        return pltpu.make_async_copy(
            source.at[s], target.at[s, :, window(t, width)], own_sem.at[kind]
        )

    def to_expert(kind, m):
        source, target = kinds[kind]
        q = flip(s, m)
        return remote(
            source.at[q], target.at[s, :, window(t, width)], sa.at[kind, m], ra.at[kind, m], (q, t)
        )

    def share(kind, m, k):
        bit = low_bit(k)
        block = kinds[kind][1].at[flip(s, m), :, window(flip(t, k - bit), width)]
        return remote(block, block, st.at[kind, m, k], rt.at[kind, m, k], (s, flip(t, bit)))

    seen = set()

    def forward(m):
        for kind in range(2):
            for k in relays_of(n_tp):
                before = k - low_bit(k)
                if (kind, m, before) not in seen:
                    share(kind, m, before).wait_recv()
                    seen.add((kind, m, before))
                share(kind, m, k).start()

    for kind in range(2):
        own(kind).start()
    for m in range(1, n_sp):
        for kind in range(2):
            to_expert(kind, m).start()
    for m in range(n_sp):
        for kind in range(2):
            if m == 0:
                own(kind).wait()
            else:
                to_expert(kind, m).wait_recv()
            for bit in bits_of(n_tp):
                share(kind, m, bit).start()
        if m > 0:
            forward(m - 1)
    forward(n_sp - 1)
    for kind in range(2):
        for m in range(n_sp):
            if m > 0:
                to_expert(kind, m).wait_send()
            for k in range(1, n_tp):
                share(kind, m, k).wait_send()
                if (kind, m, k) not in seen:
                    share(kind, m, k).wait_recv()


def combine_kernel(
    n_sp, n_tp, part, mixed, base, pick, out, mixed_all, half, xsend, xrecv, back, ret,
    own_sem, sh, rh, sx, rx, sb, rb, sg, rg, st, rt,
):
    s, t = lax.axis_index("sp"), lax.axis_index("tp")
    width = ret.shape[-1]
    pair, across = flip(t, 1), flip(t, 2)
    greet(
        [(flip(s, m), t) for m in range(1, n_sp)] + [(s, flip(t, b)) for b in bits_of(n_tp)]
    )

    def to_pair(slot):
        chunk = flip(pair, 2) if slot == 0 else pair
        return remote(
            part.at[:, :, window(chunk, width)], half.at[slot], sh.at[slot], rh.at[slot], (s, pair)
        )

    def cross(m):
        q = flip(s, m)
        return remote(xsend.at[q], xrecv.at[q], sx.at[m], rx.at[m], (s, across))

    def give(m):
        q = flip(s, m)
        return remote(back.at[q], ret.at[s], sb.at[m], rb.at[m], (q, t))

    def gather(k):
        bit = low_bit(k)
        block = flip(s, k - bit)
        source = mixed if k == bit else mixed_all.at[block]
        return remote(source, mixed_all.at[block], sg.at[k], rg.at[k], (flip(s, bit), t))

    seen = set()

    def forward(masks):
        for k in masks:
            before = k - low_bit(k)
            if before not in seen:
                gather(before).wait_recv()
                seen.add(before)
            gather(k).start()

    to_pair(0).start()
    to_pair(1).start()
    own = pltpu.make_async_copy(mixed, mixed_all.at[s], own_sem)
    own.start()
    for bit in bits_of(n_sp):
        gather(bit).start()
    order = list(range(n_sp - 1, -1, -1))
    to_pair(0).wait_recv()
    for m in order:
        q = flip(s, m)
        xsend[q] = (
            part[q, :, window(across, width)].astype(jnp.float32) + half[0, q].astype(jnp.float32)
        ).astype(jnp.bfloat16)
        cross(m).start()
    to_pair(1).wait_recv()
    relays = relays_of(n_sp)
    early = [k for k in relays if bin(k).count("1") == 2]
    forward(early)
    for place, m in enumerate(order):
        q = flip(s, m)
        cross(m).wait_recv()
        total = (
            part[q, :, window(t, width)].astype(jnp.float32)
            + half[1, q].astype(jnp.float32)
            + xrecv[q].astype(jnp.float32)
        ).astype(jnp.bfloat16)
        if m == 0:
            ret[s] = total
        else:
            back[q] = total
            give(m).start()
        if place == n_sp // 2:
            forward([k for k in relays if k not in early])
    total = base[...].astype(jnp.float32)
    for m in range(n_sp):
        q = flip(s, m)
        if m > 0:
            give(m).wait_recv()
        total = total + contract_rows(pick[q], ret[q])
    out[:, window(t, width)] = total.astype(jnp.bfloat16)

    def share(k):
        bit = low_bit(k)
        block = out.at[:, window(flip(t, k - bit), width)]
        return remote(block, block, st.at[k], rt.at[k], (s, flip(t, bit)))

    for bit in bits_of(n_tp):
        share(bit).start()
    shared = set()
    for k in relays_of(n_tp):
        before = k - low_bit(k)
        if before not in shared:
            share(before).wait_recv()
            shared.add(before)
        share(k).start()
    for k in range(1, n_tp):
        share(k).wait_send()
        if k not in shared:
            share(k).wait_recv()
    own.wait()
    for slot in range(2):
        to_pair(slot).wait_send()
    for m in range(n_sp):
        cross(m).wait_send()
        if m > 0:
            give(m).wait_send()
            gather(m).wait_send()
            if m not in seen:
                gather(m).wait_recv()


def scan_kernel(
    n_sp, flipped, drive, decay, state_grad, pieces, weight, carry, carries,
    own_sem, sa, ra, sc, rc,
):
    s, t = lax.axis_index("sp"), lax.axis_index("tp")
    rows = drive.shape[0]
    share = flipped.shape[0] // n_sp
    greet([(flip(s, m), t) for m in range(1, n_sp)])

    def piece(m):
        q = flip(s, m)
        return remote(
            flipped.at[window(q, share)], pieces.at[:, window(s, rows)], sa.at[m], ra.at[m], (q, t)
        )

    def send_carry(m):
        return remote(carry, carries.at[s], sc.at[m], rc.at[m], (flip(s, m), t))

    own = pltpu.make_async_copy(
        flipped.at[window(s, share)], pieces.at[:, window(s, rows)], own_sem
    )
    own.start()

    def lap(step, held):
        grad, product = held
        row = rows - 1 - step
        grad = drive[pl.ds(row, 1), :] + grad
        product_here = product
        state_grad[pl.ds(row, 1), :] = grad
        weight[pl.ds(row, 1), :] = product_here
        now = decay[pl.ds(row, 1), :]
        return (now * grad, now * product_here)

    zero = jnp.zeros((1, drive.shape[1]), jnp.float32)
    start, span = lax.fori_loop(0, rows, lap, (zero, zero + 1.0), unroll=8)
    carry[0:1, :] = span
    carry[1:2, :] = start
    for m in range(1, n_sp):
        send_carry(m).start()
    for m in range(1, n_sp):
        piece(m).start()
    for m in range(1, n_sp):
        send_carry(m).wait_recv()
    incoming = zero
    for later in range(n_sp - 1, 0, -1):
        longer = carries[later, 1:2, :] + carries[later, 0:1, :] * incoming
        incoming = jnp.where(later > s, longer, incoming)
    state_grad[...] = state_grad[...] + weight[...] * incoming
    own.wait()
    for m in range(1, n_sp):
        send_carry(m).wait_send()
        piece(m).wait_send()
        piece(m).wait_recv()


def silu_parts(values):
    sig = jax.nn.sigmoid(values)
    return (values * sig, sig * (1.0 + values * (1.0 - sig)))


def route_slots(route_block, experts, capacity):
    flat_ids = route_block.reshape(-1)
    onehot = (flat_ids[:, None] == jnp.arange(experts, dtype=jnp.int32)[None, :]).astype(jnp.int32)
    before = jnp.cumsum(onehot, axis=0) - onehot
    slot_rank = jnp.sum(before * onehot, axis=1)
    return flat_ids * capacity + slot_rank


def contract_rows(left, right):
    return lax.dot_general(
        left, right, (((0,), (0,)), ((), ())), preferred_element_type=jnp.float32
    )


def sparse_body(
    cotangent,
    mixer_out,
    route_ids,
    route_weights,
    conv_out,
    recur_gate,
    input_gate,
    gate_pre,
    states_before,
    decay_rate,
    out_proj,
    recur_map,
    input_map,
    expert_gate,
    expert_up,
    expert_down,
):
    row_count = cotangent.shape[0]
    experts = lax.axis_size("sp")
    capacity = 4 * row_count // experts
    slot_pos = route_slots(route_ids, experts, capacity).reshape(row_count, 2)
    slot_range = jnp.arange(experts * capacity, dtype=jnp.int32)[:, None]
    hit_first = slot_range == slot_pos[None, :, 0]
    hit_second = slot_range == slot_pos[None, :, 1]
    dispatch = (hit_first | hit_second).astype(jnp.bfloat16)
    slot_weight = jnp.sum(
        jnp.where(hit_first, route_weights[None, :, 0], 0.0)
        + jnp.where(hit_second, route_weights[None, :, 1], 0.0),
        axis=1,
    )
    send_rows = jnp.dot(dispatch, mixer_out, preferred_element_type=jnp.float32).astype(
        jnp.bfloat16
    )
    send_cot = (
        jnp.dot(dispatch, cotangent, preferred_element_type=jnp.float32) * slot_weight[:, None]
    ).astype(jnp.bfloat16)
    tps = lax.axis_size("tp")
    features = tps * cotangent.shape[1]
    slots = experts * capacity
    blocks = (experts, capacity, features)
    got_rows, got_cot = call(
        functools.partial(dispatch_kernel, experts, tps),
        [jax.ShapeDtypeStruct(blocks, jnp.bfloat16)] * 2,
        [
            DMA((2,)),
            DMA((2, experts)),
            DMA((2, experts)),
            DMA((2, experts, tps)),
            DMA((2, experts, tps)),
        ],
        0,
        send_rows.reshape(experts, capacity, -1),
        send_cot.reshape(experts, capacity, -1),
    )
    got_rows, got_cot = (got_rows.reshape(slots, features), got_cot.reshape(slots, features))
    w_gate = expert_gate[0]
    w_up = expert_up[0]
    w_down = expert_down[0]
    pre_gate = jnp.dot(got_rows, w_gate, preferred_element_type=jnp.float32)
    pre_up = jnp.dot(got_rows, w_up, preferred_element_type=jnp.float32)
    gate_act, slope = silu_parts(pre_gate)
    active = (gate_act * pre_up).astype(jnp.bfloat16)
    d_active = lax.dot_general(
        got_cot, w_down, (((1,), (1,)), ((), ())), preferred_element_type=jnp.float32
    )
    grad_down = contract_rows(active, got_cot).astype(jnp.bfloat16)
    d_gate = (d_active * pre_up * slope).astype(jnp.bfloat16)
    d_up = (d_active * gate_act).astype(jnp.bfloat16)
    grad_gate = contract_rows(got_rows, d_gate).astype(jnp.bfloat16)
    grad_up = contract_rows(got_rows, d_up).astype(jnp.bfloat16)
    partial_grad = lax.dot_general(
        d_gate, w_gate, (((1,), (1,)), ((), ())), preferred_element_type=jnp.float32
    ) + lax.dot_general(d_up, w_up, (((1,), (1,)), ((), ())), preferred_element_type=jnp.float32)
    channels = conv_out.shape[1]
    rate = decay_rate[None, :]
    recur_f = recur_gate.astype(jnp.float32)
    input_f = input_gate.astype(jnp.float32)
    conv_f = conv_out.astype(jnp.float32)
    before_f = states_before.astype(jnp.float32)
    log_decay = -8.0 * recur_f * rate
    decay_now = jnp.exp(log_decay)
    position = lax.axis_index("sp") * row_count + jnp.arange(row_count, dtype=jnp.int32)
    at_start = (position == 0)[:, None]
    norm_factor = jnp.where(at_start, 1.0, jnp.sqrt(-jnp.expm1(2.0 * log_decay)))
    norm_slope = jnp.where(at_start, 0.0, -jnp.exp(2.0 * log_decay) / norm_factor)
    drive = input_f * conv_f
    state = decay_now * before_f + norm_factor * drive
    gate, gelu_back = jax.vjp(jax.nn.gelu, gate_pre.astype(jnp.float32))
    mixed = (state * gate).astype(jnp.bfloat16)
    block = (experts, capacity, cotangent.shape[1])
    pair_sems, own_sems = (DMA((2,)), DMA((experts,)))
    tp_sems = DMA((tps,))
    out_grad, mixed_all = call(
        functools.partial(combine_kernel, experts, tps),
        [
            jax.ShapeDtypeStruct((row_count, features), jnp.bfloat16),
            jax.ShapeDtypeStruct((experts, row_count, channels), jnp.bfloat16),
        ],
        [
            pltpu.VMEM((2, *block), jnp.bfloat16),
            pltpu.VMEM(block, jnp.bfloat16),
            pltpu.VMEM(block, jnp.bfloat16),
            pltpu.VMEM(block, jnp.bfloat16),
            pltpu.VMEM(block, jnp.bfloat16),
            DMA,
            pair_sems,
            pair_sems,
            *([own_sems] * 6),
            tp_sems,
            tp_sems,
        ],
        1,
        partial_grad.astype(jnp.bfloat16).reshape(blocks),
        mixed,
        cotangent,
        dispatch.reshape(experts, capacity, row_count),
    )
    d_mixed = jnp.dot(out_grad, out_proj, preferred_element_type=jnp.float32)
    state_grad, pieces = call(
        functools.partial(scan_kernel, experts),
        [
            jax.ShapeDtypeStruct((row_count, channels), jnp.float32),
            jax.ShapeDtypeStruct((features // experts, experts * row_count), jnp.bfloat16),
        ],
        [
            pltpu.VMEM((row_count, channels), jnp.float32),
            pltpu.VMEM((2, channels), jnp.float32),
            pltpu.VMEM((experts, 2, channels), jnp.float32),
            DMA,
            *([own_sems] * 4),
        ],
        2,
        out_grad.T,
        d_mixed * gate,
        decay_now,
    )
    grad_out_proj = jnp.dot(
        pieces,
        mixed_all.reshape(experts * row_count, channels),
        preferred_element_type=jnp.float32,
    )
    grad_gate_pre = gelu_back(d_mixed * state)[0].astype(jnp.bfloat16)
    d_log = state_grad * (decay_now * before_f + norm_slope * drive)
    d_recur_pre = (d_log * (-8.0 * rate) * recur_f * (1.0 - recur_f)).astype(jnp.bfloat16)
    d_input_pre = (state_grad * norm_factor * conv_f * input_f * (1.0 - input_f)).astype(
        jnp.bfloat16
    )
    groups = recur_map.shape[0]
    width = recur_map.shape[1]
    through_recur = jnp.einsum(
        "tbj,bij->tbi",
        d_recur_pre.reshape(row_count, groups, width),
        recur_map,
        preferred_element_type=jnp.float32,
    )
    through_input = jnp.einsum(
        "tbj,bij->tbi",
        d_input_pre.reshape(row_count, groups, width),
        input_map,
        preferred_element_type=jnp.float32,
    )
    grad_conv = (
        state_grad * norm_factor * input_f
        + (through_recur + through_input).reshape(row_count, channels)
    ).astype(jnp.bfloat16)
    return (
        grad_gate[None],
        grad_up[None],
        grad_down[None],
        grad_out_proj,
        grad_conv,
        grad_gate_pre,
    )


def body(
    cotangent,
    mixer_out,
    route_ids,
    route_weights,
    conv_out,
    recur_gate,
    input_gate,
    gate_pre,
    states_before,
    decay_rate,
    out_proj,
    recur_map,
    input_map,
    expert_gate,
    expert_up,
    expert_down,
):
    experts, tps = lax.axis_size("sp"), lax.axis_size("tp")
    row_count = cotangent.shape[0]
    capacity = 4 * row_count // experts
    if 2 * capacity < row_count:
        return sparse_body(
            cotangent,
            mixer_out,
            route_ids,
            route_weights,
            conv_out,
            recur_gate,
            input_gate,
            gate_pre,
            states_before,
            decay_rate,
            out_proj,
            recur_map,
            input_map,
            expert_gate,
            expert_up,
            expert_down,
        )
    grad_out_proj, grad_gate, grad_up, grad_down, grad_conv, grad_gate_pre = run_dense(
        experts,
        tps,
        capacity,
        mixer_out,
        cotangent,
        route_ids.T,
        route_weights.T,
        conv_out,
        recur_gate,
        input_gate,
        gate_pre,
        states_before,
        decay_rate[None, :],
        out_proj,
        expert_gate[0],
        expert_up[0],
        expert_down[0],
        recur_map,
        input_map,
    )
    return (
        grad_gate[None],
        grad_up[None],
        grad_down[None],
        grad_out_proj,
        grad_conv,
        grad_gate_pre,
    )


def solution(mesh):
    placed = (
        P("sp", "tp"),
        P("sp", "tp"),
        P("sp", None),
        P("sp", None),
        P("sp", "tp"),
        P("sp", "tp"),
        P("sp", "tp"),
        P("sp", "tp"),
        P("sp", "tp"),
        P("tp"),
        P(None, "tp"),
        P("tp", None, None),
        P("tp", None, None),
        P("sp", None, "tp"),
        P("sp", None, "tp"),
        P("sp", "tp", None),
    )
    return jax.shard_map(
        body,
        mesh=mesh,
        in_specs=placed,
        out_specs=(
            P("sp", None, "tp"),
            P("sp", None, "tp"),
            P("sp", "tp", None),
            P("sp", "tp"),
            P("sp", "tp"),
            P("sp", "tp"),
        ),
        check_vma=False,
    )
```

```python
import functools

import jax
import jax.numpy as jnp
from jax import lax
from jax.experimental import pallas as pl
from jax.experimental.pallas import tpu as pltpu
from jax.sharding import PartitionSpec as P

MESH = pl.DeviceIdType.MESH
VMEM = pl.BlockSpec(memory_space=pltpu.VMEM)
DMA = pltpu.SemaphoreType.DMA


def bits_of(count):
    found, bit = [], 1
    while bit < count:
        found.insert(0, bit)
        bit *= 2
    return found


def low_bit(mask):
    return mask & -mask


def flip(index, mask):
    bit = 1
    while bit <= mask:
        if mask & bit:
            index = index + bit - 2 * bit * lax.rem(lax.div(index, bit), 2)
        bit *= 2
    return index


def window(index, width):
    return pl.ds(pl.multiple_of(index * width, width), width)


def remote(source, target, send_sem, recv_sem, device):
    return pltpu.make_async_remote_copy(
        src_ref=source,
        dst_ref=target,
        send_sem=send_sem,
        recv_sem=recv_sem,
        device_id=device,
        device_id_type=MESH,
    )


def greet(peers):
    barrier = pltpu.get_barrier_semaphore()
    for peer in peers:
        pl.semaphore_signal(barrier, inc=1, device_id=peer, device_id_type=MESH)
    pl.semaphore_wait(barrier, len(peers))


def relays_of(count):
    masks = [mask for mask in range(1, count) if mask != low_bit(mask)]
    return sorted(masks, key=lambda mask: (bin(mask).count("1"), -mask))


def call(kernel, out_shape, scratch, ident, *operands):
    return pl.pallas_call(
        kernel,
        out_shape=out_shape,
        in_specs=[VMEM] * len(operands),
        out_specs=jax.tree.map(lambda _: VMEM, out_shape),
        scratch_shapes=scratch,
        compiler_params=pltpu.CompilerParams(
            collective_id=ident, has_side_effects=True, vmem_limit_bytes=48 * 1024 * 1024
        ),
    )(*operands)


def along(index, table):
    found = 0
    for place, value in enumerate(table):
        found = found + jnp.where(index == place, value, 0)
    return found


def abs_of(value):
    return jnp.where(value < 0, -value, value)


def nearest(count):
    return [sorted(range(count), key=lambda other: (abs(other - z), other)) for z in range(count)]


def contract_columns(left, right):
    return lax.dot_general(
        left, right, (((1,), (1,)), ((), ())), preferred_element_type=jnp.float32
    )


def expm1_of(values):
    near = 1.0 / 362880.0
    for factor in (40320.0, 5040.0, 720.0, 120.0, 24.0, 6.0, 2.0, 1.0):
        near = near * values + 1.0 / factor
    return jnp.where(jnp.abs(values) < 0.3, values * near, jnp.exp(values) - 1.0)


def expert_kernel(
    n_sp, n_tp, capacity,
    rows_hbm, cots_hbm, ids_hbm, weights_hbm, conv_hbm, recur_hbm, input_hbm, gate_hbm,
    before_hbm, rate_hbm, proj_hbm, w_gate_hbm, w_up_hbm, w_down_hbm, recur_map_hbm,
    input_map_hbm,
    proj_block, grad_gate, grad_up, grad_down, grad_conv, grad_gate_pre,
    rows, cots, ids, weights, conv, recur, inputs, gate_pre, before, rate, proj,
    w_gate, w_up, w_down, recur_map, input_map,
    tok, meta, got, ybuf, act, dgate, dup, give_pair, mine, half,
    xsend, xrecv, back, ret, pick, mixed_all, pieces, out, mixed, decay, gate, gate_part, drive, product,
    state_grad, recur_part, input_part, conv_part, carry, carries,
    lsem, tss, trs, mss, mrs, yss, yrs, hss, hrs, hds, pss, prs, css, crs, gss, grs,
    zss, zrs, oss, ors, iss, irs, kss, krs, own_sem,
):
    s, t = lax.axis_index("sp"), lax.axis_index("tp")
    n_y = 2
    n_z = n_sp // n_y
    z, y = lax.div(s, n_y), lax.rem(s, n_y)
    beside = flip(s, 1)
    pair, across = flip(t, 1), flip(t, 2)
    tokens, width = rows.shape
    chunk = n_y * capacity
    f32, bf16 = jnp.float32, jnp.bfloat16
    order = [along(z, [found[k] for found in nearest(n_z)]) for k in range(n_z)]

    fetch = [
        pltpu.make_async_copy(source, target, lsem.at[i])
        for i, (source, target) in enumerate(
            (
                (rows_hbm, rows), (cots_hbm, cots), (ids_hbm, ids), (weights_hbm, weights),
                (conv_hbm, conv), (recur_hbm, recur), (input_hbm, inputs), (gate_hbm, gate_pre),
                (before_hbm, before), (rate_hbm, rate),
                (w_gate_hbm, w_gate), (w_up_hbm, w_up), (w_down_hbm, w_down), (proj_hbm, proj),
                (recur_map_hbm, recur_map), (input_map_hbm, input_map),
            )
        )
    ]
    for copy in fetch:
        copy.start()
    barrier_peers = [(flip(s, m), t) for m in range(1, n_sp)]
    barrier_peers += [(flip(s, m), flip(t, 2)) for m in range(1, n_sp)]
    greet(barrier_peers + [(s, flip(t, b)) for b in bits_of(n_tp)])
    for copy in fetch[:4]:
        copy.wait()
    ends = []

    def begin(copy, valid=None, alone=True):
        if alone:
            ends.append((copy, valid))
        if valid is None:
            copy.start()
        else:
            pl.when(valid)(copy.start)

    def spread(make, zb, first):
        above, below = z + 1 < n_z, z >= 1
        if not first:
            above, below = (zb < z) & above, (zb > z) & below
        begin(make(zb, z + 1, 0), above)
        begin(make(zb, z - 1, 1), below)

    def along_line(source, target, send_sem, recv_sem, z_to):
        return remote(source, target, send_sem, recv_sem, (z_to * n_y + y, t))

    def move_tokens(kind, zb, z_to, way, own):
        target = tok.at[kind, zb]
        source = (rows, cots)[kind] if own else target
        return along_line(source, target, tss.at[kind, zb, way], trs.at[kind, zb], z_to)

    def move_meta(zb, z_to, way):
        return along_line(meta.at[zb], meta.at[zb], mss.at[zb, way], mrs.at[zb], z_to)

    def move_mixed(zb, z_to, way, own):
        target = mixed_all.at[zb * n_y + y]
        source = mixed if own else target
        return along_line(source, target, zss.at[zb, way], zrs.at[zb * n_y + y], z_to)

    def mixed_beside(zb, own):
        target = mixed_all.at[zb * n_y + y]
        source = mixed if own else target
        return remote(source, target, zss.at[zb, 2], zrs.at[zb * n_y + y], (beside, t))

    def mixed_from_beside(zb):
        target = mixed_all.at[zb * n_y + 1 - y]
        return remote(mixed, target, zss.at[zb, 2], zrs.at[zb * n_y + 1 - y], (beside, t))

    def slots(kind, block, quarter):
        return got.at[kind, window(block, capacity), window(quarter, width)]

    def to_beside(kind, zb):
        return remote(
            ybuf.at[kind, zb], slots(kind, zb * n_y + y, t),
            yss, yrs.at[kind, zb], (beside, t),
        )

    def from_beside(kind, zb):
        return remote(
            ybuf.at[kind, zb], slots(kind, zb * n_y + 1 - y, t),
            yss, yrs.at[kind, zb], (beside, t),
        )

    def share(kind, block, k):
        bit = low_bit(k)
        ref = slots(kind, block, flip(t, k - bit))
        recv_sem = hrs.at[kind, block] if k == 2 else hds.at[lax.div(block, n_y)]
        return remote(ref, ref, hss, recv_sem, (s, flip(t, bit)))

    def crossed(kind, block):
        ref = slots(kind, block, across)
        return remote(ref, ref, hss, hrs.at[kind, block], (s, across))

    table_rows = lax.broadcasted_iota(jnp.int32, (2 * n_sp, tokens), 0)
    first_id, second_id = ids[0:1, :], ids[1:2, :]
    hits = ((first_id == table_rows) | (second_id == table_rows)).astype(f32)
    earlier = lax.broadcasted_iota(jnp.int32, (tokens, tokens), 0) < lax.broadcasted_iota(
        jnp.int32, (tokens, tokens), 1
    )
    rank = jnp.dot(
        hits.astype(bf16), earlier.astype(f32).astype(bf16), preferred_element_type=f32
    )
    rank = jnp.where(hits > 0.0, rank, -1.0)
    weight_rows = table_rows - n_sp
    weight = jnp.where(first_id == weight_rows, weights[0:1, :], 0.0) + jnp.where(
        second_id == weight_rows, weights[1:2, :], 0.0
    )
    meta[z] = jnp.where(table_rows < n_sp, rank, weight)

    spread(lambda zb, to, way: move_tokens(0, zb, to, way, True), z, True)
    spread(move_meta, z, True)
    spread(lambda zb, to, way: move_tokens(1, zb, to, way, True), z, True)

    slot_index = lax.broadcasted_iota(jnp.int32, (capacity, tokens), 0).astype(f32)

    def chosen(zb, expert):
        return meta[zb, pl.ds(expert, 1), :] == slot_index

    def compact(kind, k, valid=None):
        zb = order[k]
        block = zb * n_y + y
        sends = (to_beside(kind, zb), share(kind, block, 2), share(kind, block, 1))

        def work():
            picks = jnp.concatenate(
                [chosen(zb, s).astype(f32), chosen(zb, beside).astype(f32)], axis=0
            )
            source = tok[kind, zb] if k > 0 else (rows, cots)[kind][...]
            found = jnp.dot(picks.astype(bf16), source, preferred_element_type=f32)
            if kind == 1:
                table = jnp.concatenate(
                    [
                        jnp.broadcast_to(meta[zb, pl.ds(n_sp + e, 1), :], (capacity, tokens))
                        for e in (s, beside)
                    ],
                    axis=0,
                )
                found = found * jnp.sum(picks * table, axis=1, keepdims=True)
            found = found.astype(bf16)
            ybuf[kind, zb] = found[capacity:]
            got[kind, window(block, capacity), window(t, width)] = found[:capacity]
            for copy in sends:
                copy.start()

        if valid is None:
            work()
        else:
            pl.when(valid)(work)

    def hear(distance, kind):
        for k in range(1, n_z):
            apart = {abs(found[k] - place) for place, found in enumerate(nearest(n_z))}
            if distance not in apart:
                continue
            zb = order[k]
            only = None if len(apart) == 1 else abs_of(zb - z) == distance
            waits = [move_tokens(kind, zb, z, 0, False)] + [move_meta(zb, z, 0)] * (kind == 0)
            for copy in waits:
                if only is None:
                    copy.wait_recv()
                else:
                    pl.when(only)(copy.wait_recv)
            make = [lambda zb, to, way: move_tokens(kind, zb, to, way, False)]
            for made in make + [move_meta] * (kind == 0):
                above, below = (zb < z) & (z + 1 < n_z), (zb > z) & (z >= 1)
                if only is not None:
                    above, below = above & only, below & only
                begin(made(zb, z + 1, 0), above)
                begin(made(zb, z - 1, 1), below)
        for k in range(1, n_z):
            apart = {abs(found[k] - place) for place, found in enumerate(nearest(n_z))}
            if distance in apart:
                only = None if len(apart) == 1 else abs_of(order[k] - z) == distance
                compact(kind, k, only)

    def take_beside(kind, k):
        block = order[k] * n_y + 1 - y
        from_beside(kind, order[k]).wait_recv()
        begin(share(kind, block, 2), alone=False)
        begin(share(kind, block, 1), alone=False)

    def relay_x(kind, k):
        for block in (order[k] * n_y + y, order[k] * n_y + 1 - y):
            crossed(kind, block).wait_recv()
            begin(share(kind, block, 3), alone=False)

    def gather_chunk(k):
        both = got.at[:, window(order[k], chunk), pl.ds(0, (n_tp // 2) * width)]
        remote(both, both, hss, hds.at[order[k]], (s, pair)).wait_recv()

    def to_pair(zb, slot):
        here = window(zb, chunk)
        return remote(
            give_pair.at[slot, here], half.at[slot, here],
            pss, prs.at[zb, slot], (s, pair),
        )

    def cross(zb):
        here = window(zb, chunk)
        return remote(xsend.at[here], xrecv.at[here], css, crs.at[zb], (s, across))

    def give(block):
        here = window(block, capacity)
        return remote(
            back.at[here], ret.at[window(s, capacity)], gss, grs, (block, t)
        )

    def given():
        most = pl.ds(0, (n_sp - 1) * capacity)
        return remote(back.at[most], ret.at[most], gss, grs, (beside, t))

    def experts(k):
        zb = order[k]
        here = window(zb, chunk)
        got_rows = got[0, here, :]
        pre_gate = jnp.dot(got_rows, w_gate[...], preferred_element_type=f32)
        pre_up = jnp.dot(got_rows, w_up[...], preferred_element_type=f32)
        d_active = contract_columns(got[1, here, :], w_down[...])
        gate_act, slope = silu_parts(pre_gate)
        act[here, :] = (gate_act * pre_up).astype(bf16)
        d_gate = (d_active * pre_up * slope).astype(bf16)
        d_up = (d_active * gate_act).astype(bf16)
        dgate[here, :] = d_gate
        dup[here, :] = d_up

        def partial(quarter):
            columns = window(quarter, width)
            return contract_columns(d_gate, w_gate[columns, :]) + contract_columns(
                d_up, w_up[columns, :]
            )

        give_pair[0, here, :] = partial(flip(pair, 2)).astype(bf16)
        begin(to_pair(zb, 0), alone=False)
        give_pair[1, here, :] = partial(pair).astype(bf16)
        begin(to_pair(zb, 1), alone=False)
        mine[0, here, :] = partial(across)
        mine[1, here, :] = partial(t)

    def send_across(k):
        zb = order[k]
        here = window(zb, chunk)
        to_pair(zb, 0).wait_recv()
        xsend[here, :] = (mine[0, here, :] + half[0, here, :].astype(f32)).astype(bf16)
        begin(cross(zb), alone=False)

    def send_home(k):
        zb = order[k]
        here = window(zb, chunk)
        to_pair(zb, 1).wait_recv()
        cross(zb).wait_recv()
        total = (
            mine[1, here, :] + half[1, here, :].astype(f32) + xrecv[here, :].astype(f32)
        ).astype(bf16)
        back[here, :] = total
        if k > 0:
            begin(give(zb * n_y + y), alone=False)
        else:
            ret[window(s, capacity), :] = back[window(s, capacity), :]
        begin(give(zb * n_y + 1 - y), alone=False)

    step = 256 if width % 256 == 0 else width

    def weight_grad(target, kind, right):
        def lap(j, _):
            columns = window(j, step)
            target[columns, :] = contract_rows(got[kind, :, columns], right[...]).astype(bf16)
            return 0

        lax.fori_loop(0, n_tp * width // step, lap, 0)

    def down_grad():
        def lap(j, _):
            columns = window(j, step)
            grad_down[:, columns] = contract_rows(act[...], got[1, :, columns]).astype(bf16)
            return 0

        lax.fori_loop(0, n_tp * width // step, lap, 0)

    def send_mixed():
        spread(lambda zb, to, way: move_mixed(zb, to, way, True), z, True)
        begin(mixed_beside(z, True))

    def take_mixed(distance):
        for k in range(1, n_z):
            apart = {abs(found[k] - place) for place, found in enumerate(nearest(n_z))}
            if distance not in apart:
                continue
            zb = order[k]
            only = None if len(apart) == 1 else abs_of(zb - z) == distance
            wait = move_mixed(zb, z, 0, False).wait_recv
            if only is None:
                wait()
            else:
                pl.when(only)(wait)
            above, below = (zb < z) & (z + 1 < n_z), (zb > z) & (z >= 1)
            if only is not None:
                above, below = above & only, below & only
            begin(move_mixed(zb, z + 1, 0, False), above)
            begin(move_mixed(zb, z - 1, 1, False), below)
            begin(mixed_beside(zb, False), only)

    def share_out(k):
        bit = low_bit(k)
        ref = out.at[:, window(flip(t, k - bit), width)]
        return remote(ref, ref, oss, ors.at[k - 1], (s, flip(t, bit)))

    def out_arrived(k):
        ref = out.at[:, window(flip(t, k), width)]
        return remote(ref, ref, oss, ors.at[k - 1], (s, flip(t, low_bit(k))))

    strip = 16

    def recurrence():
        def lap(j, _):
            here = window(j, strip)
            rate_row = rate[...]
            recur_f = recur[here, :].astype(f32)
            input_f = inputs[here, :].astype(f32)
            conv_f = conv[here, :].astype(f32)
            before_f = before[here, :].astype(f32)
            gate_f = gate_pre[here, :].astype(f32)
            log_decay = -8.0 * recur_f * rate_row
            decay_now = jnp.exp(log_decay)
            place = lax.broadcasted_iota(jnp.int32, conv_f.shape, 0) + (s * tokens + j * strip)
            at_start = place == 0
            norm = jnp.where(at_start, 1.0, jnp.sqrt(-expm1_of(2.0 * log_decay)))
            slope = jnp.where(at_start, 0.0, -jnp.exp(2.0 * log_decay) / norm)
            entry = input_f * conv_f
            kept = decay_now * before_f
            state = kept + norm * entry
            inner = 0.7978845608028654 * (gate_f + 0.044715 * gate_f * gate_f * gate_f)
            bend = jnp.tanh(inner)
            half_up = 0.5 * (1.0 + bend)
            gate_now = gate_f * half_up
            gate_slope = half_up + 0.5 * gate_f * (1.0 - bend * bend) * 0.7978845608028654 * (
                1.0 + 3.0 * 0.044715 * gate_f * gate_f
            )
            decay[here, :] = decay_now
            gate[here, :] = gate_now
            gate_part[here, :] = state * gate_slope
            mixed[here, :] = (state * gate_now).astype(bf16)
            recur_part[here, :] = (
                (kept + slope * entry) * (-8.0 * rate_row) * recur_f * (1.0 - recur_f)
            )
            input_part[here, :] = norm * conv_f * input_f * (1.0 - input_f)
            conv_part[here, :] = norm * input_f
            return 0

        lax.fori_loop(0, tokens // strip, lap, 0)

        def back_lap(step, held):
            row = tokens - 1 - step
            product[pl.ds(row, 1), :] = held
            return held * decay[pl.ds(row, 1), :]

        one = jnp.ones((1, width), f32)
        carry[0:1, :] = lax.fori_loop(0, tokens, back_lap, one, unroll=8)

    cut = n_tp * width // n_sp
    held_blocks = width // cut

    def piece(j, way):
        q = t * held_blocks + j
        return remote(
            out.at[:, window(q, cut)], pieces.at[s], iss.at[j, way], irs.at[s],
            (q, across if way else t),
        )

    def piece_beside(block):
        return remote(
            pieces.at[block], pieces.at[block], kss, irs.at[block], (s, pair)
        )

    def send_carry(m):
        return remote(carry, carries.at[s], krs.at[0, m], krs.at[1, m], (flip(s, m), t))

    for kind in range(2):
        compact(kind, 0)
    for expert in range(n_sp):
        pick[expert * capacity : (expert + 1) * capacity, :] = (
            chosen(z, expert).astype(f32).astype(bf16)
        )
    for kind in range(2):
        take_beside(kind, 0)
    hear(1, 0)
    hear(1, 1)
    take_beside(0, 1)
    for copy in fetch[4:]:
        copy.wait()
    recurrence()
    own_mixed = pltpu.make_async_copy(mixed, mixed_all.at[s], own_sem)
    own_mixed.start()
    relay_x(0, 0)
    relay_x(1, 0)
    for distance in range(2, n_z):
        hear(distance, 0)
        take_beside(1, distance - 1)
        hear(distance, 1)
        if distance == n_z - 2:
            send_mixed()
        if distance == 2:
            gather_chunk(0)
            experts(0)
        take_beside(0, distance)
        for kind in range(2):
            relay_x(kind, distance - 1)
    take_beside(1, n_z - 1)
    take_mixed(1)
    send_across(0)
    for k in range(n_z - 2, n_z):
        gather_chunk(k)
        experts(k)
        if k == n_z - 2:
            for kind in range(2):
                relay_x(kind, n_z - 1)
        send_across(k)
    for distance in range(2, n_z - 1):
        take_mixed(distance)
    send_home(n_z - 2)
    send_home(0)
    for k in range(1, n_z - 2):
        gather_chunk(k)
        experts(k)
        send_across(k)
    send_home(n_z - 1)
    down_grad()
    for k in range(1, n_z - 2):
        send_home(k)
    weight_grad(grad_gate, 0, dgate)
    weight_grad(grad_up, 0, dup)
    take_mixed(n_z - 1)
    given().wait_recv()
    total = cots[...].astype(f32) + contract_rows(pick[...], ret[...])
    out[:, window(t, width)] = total.astype(bf16)
    begin(share_out(2), alone=False)
    begin(share_out(1), alone=False)
    for j in range(held_blocks):
        q = t * held_blocks + j
        begin(piece(j, 0), abs_of(q - s) > 0)
        begin(piece(j, 1), abs_of(q - s) > 0)

    def through_proj(k):
        columns = window(flip(t, k), width)
        return jnp.dot(out[:, columns], proj[columns, :], preferred_element_type=f32)

    drive[...] = through_proj(0)
    out_arrived(1).wait_recv()
    drive[...] += through_proj(1)
    out_arrived(2).wait_recv()
    begin(share_out(3), alone=False)
    drive[...] += through_proj(2)
    out_arrived(3).wait_recv()
    d_mixed = drive[...] + through_proj(3)
    grad_gate_pre[...] = (d_mixed * gate_part[...]).astype(bf16)
    drive[...] = d_mixed * gate[...]

    def lap(step, held):
        row = tokens - 1 - step
        grad = drive[pl.ds(row, 1), :] + held
        state_grad[pl.ds(row, 1), :] = grad
        return decay[pl.ds(row, 1), :] * grad

    zero = jnp.zeros((1, width), f32)
    carry[1:2, :] = lax.fori_loop(0, tokens, lap, zero, unroll=8)
    direct = lax.rem(lax.div(s, held_blocks), 2) == lax.rem(t, 2)
    for m in range(1, n_sp):
        begin(send_carry(m), flip(s, m) < s)
    pieces[s] = out[:, window(s, cut)]
    for m in range(1, n_sp):
        block = flip(s, m)
        pl.when(direct)(piece_beside(block).wait_recv)
        begin(piece_beside(block), direct, alone=False)
    for k in range(n_z):
        mixed_from_beside(order[k]).wait_recv()
    own_mixed.wait()
    for m in range(1, n_sp):
        pl.when(jnp.logical_not(direct))(piece_beside(flip(s, m)).wait_recv)
    proj_block[...] = contract_rows(
        pieces[...].reshape(n_sp * tokens, cut), mixed_all[...].reshape(n_sp * tokens, width)
    )
    for m in range(1, n_sp):
        pl.when(flip(s, m) > s)(send_carry(m).wait_recv)
    incoming = zero
    for later in range(n_sp - 1, 0, -1):
        longer = carries[later, 1:2, :] + carries[later, 0:1, :] * incoming
        incoming = jnp.where(later > s, longer, incoming)
    grad = state_grad[...] + product[...] * incoming
    d_recur = (grad * recur_part[...]).astype(bf16)
    d_input = (grad * input_part[...]).astype(bf16)
    straight = grad * conv_part[...]
    side = recur_map.shape[1]
    for group in range(recur_map.shape[0]):
        columns = slice(group * side, (group + 1) * side)
        through = contract_columns(d_recur[:, columns], recur_map[group])
        through = through + contract_columns(d_input[:, columns], input_map[group])
        grad_conv[:, columns] = (straight[:, columns] + through).astype(bf16)
    some = got.at[:, pl.ds(0, (n_tp - 1) * chunk), :]
    remote(some, some, hss, hds.at[0], (s, pair)).wait_send()
    remote(ybuf, ybuf, yss, yrs.at[0, 0], (beside, t)).wait_send()
    remote(give_pair, half, pss, prs.at[0, 0], (s, pair)).wait_send()
    remote(xsend, xrecv, css, crs.at[0], (s, across)).wait_send()
    given().wait_send()
    others = out.at[:, pl.ds(0, (n_tp - 1) * width)]
    remote(others, others, oss, ors.at[0], (s, pair)).wait_send()
    spare = pieces.at[pl.ds(0, n_sp - 1)]
    pl.when(direct)(remote(spare, spare, kss, irs.at[0], (s, pair)).wait_send)
    for copy, valid in ends:
        if valid is None:
            copy.wait_send()
        else:
            pl.when(valid)(copy.wait_send)


def finish_kernel(*refs):
    count = len(refs) // 2
    sems = refs[-1]
    stores = [
        pltpu.make_async_copy(refs[i], refs[count + i], sems.at[i]) for i in range(count)
    ]
    for copy in stores:
        copy.start()
    for copy in stores:
        copy.wait()


def run_dense(experts, tps, capacity, *operands):
    row_block, w_gate = operands[0], operands[11]
    tokens, width = row_block.shape
    features = tps * width
    hidden = w_gate.shape[1]
    slots, n_z = experts * capacity, experts // 2
    bf16, f32 = jnp.bfloat16, jnp.float32
    outer = pl.BlockSpec(memory_space=pltpu.HBM)
    tile, wide = (tokens, width), (tokens, features)
    cut = features // experts
    weight, down = (features, hidden), (hidden, features)
    struct = jax.ShapeDtypeStruct
    results = [
        struct((cut, width), f32),
        struct(weight, bf16),
        struct(weight, bf16),
        struct(down, bf16),
        struct(tile, bf16),
        struct(tile, bf16),
    ]
    done = pl.pallas_call(
        functools.partial(expert_kernel, experts, tps, capacity),
        out_shape=results,
        in_specs=[outer] * len(operands),
        out_specs=[VMEM] * len(results),
        scratch_shapes=[pltpu.VMEM(operand.shape, operand.dtype) for operand in operands]
        + [
            pltpu.VMEM((2, n_z, *tile), bf16),
            pltpu.VMEM((n_z, 2 * experts, tokens), f32),
            pltpu.VMEM((2, slots, features), bf16),
            pltpu.VMEM((2, n_z, capacity, width), bf16),
            pltpu.VMEM((slots, hidden), bf16),
            pltpu.VMEM((slots, hidden), bf16),
            pltpu.VMEM((slots, hidden), bf16),
            pltpu.VMEM((2, slots, width), bf16),
            pltpu.VMEM((2, slots, width), f32),
            pltpu.VMEM((2, slots, width), bf16),
            pltpu.VMEM((slots, width), bf16),
            pltpu.VMEM((slots, width), bf16),
            pltpu.VMEM((slots, width), bf16),
            pltpu.VMEM((slots, width), bf16),
            pltpu.VMEM((slots, tokens), bf16),
            pltpu.VMEM((experts, tokens, width), bf16),
            pltpu.VMEM((experts, tokens, cut), bf16),
            pltpu.VMEM(wide, bf16),
            pltpu.VMEM(tile, bf16),
            pltpu.VMEM(tile, f32),
            pltpu.VMEM(tile, f32),
            pltpu.VMEM(tile, f32),
            pltpu.VMEM(tile, f32),
            pltpu.VMEM(tile, f32),
            pltpu.VMEM(tile, f32),
            pltpu.VMEM(tile, f32),
            pltpu.VMEM(tile, f32),
            pltpu.VMEM(tile, f32),
            pltpu.VMEM((2, width), f32),
            pltpu.VMEM((experts, 2, width), f32),
            DMA((len(operands),)),
            DMA((2, n_z, 2)),
            DMA((2, n_z)),
            DMA((n_z, 2)),
            DMA((n_z,)),
            DMA,
            DMA((2, n_z)),
            DMA,
            DMA((2, experts)),
            DMA((n_z,)),
            DMA,
            DMA((n_z, 2)),
            DMA,
            DMA((n_z,)),
            DMA,
            DMA,
            DMA((n_z, 3)),
            DMA((experts,)),
            DMA,
            DMA((tps - 1,)),
            DMA((experts // tps, 2)),
            DMA((experts,)),
            DMA,
            DMA((2, experts)),
            DMA,
        ],
        compiler_params=pltpu.CompilerParams(
            collective_id=3, has_side_effects=True, vmem_limit_bytes=32 * 1024 * 1024
        ),
    )(*[pltpu.with_memory_space_constraint(each, pltpu.HBM) for each in operands])
    return pl.pallas_call(
        finish_kernel,
        out_shape=results,
        in_specs=[VMEM] * len(results),
        out_specs=[outer] * len(results),
        scratch_shapes=[DMA((len(results),))],
        compiler_params=pltpu.CompilerParams(vmem_limit_bytes=16 * 1024 * 1024),
    )(*done)


def dispatch_kernel(n_sp, n_tp, rows, cots, got_rows, got_cots, own_sem, sa, ra, st, rt):
    s, t = lax.axis_index("sp"), lax.axis_index("tp")
    width = rows.shape[-1]
    kinds = ((rows, got_rows), (cots, got_cots))
    greet(
        [(flip(s, m), t) for m in range(1, n_sp)] + [(s, flip(t, b)) for b in bits_of(n_tp)]
    )

    def own(kind):
        source, target = kinds[kind]
        return pltpu.make_async_copy(
            source.at[s], target.at[s, :, window(t, width)], own_sem.at[kind]
        )

    def to_expert(kind, m):
        source, target = kinds[kind]
        q = flip(s, m)
        return remote(
            source.at[q], target.at[s, :, window(t, width)], sa.at[kind, m], ra.at[kind, m], (q, t)
        )

    def share(kind, m, k):
        bit = low_bit(k)
        block = kinds[kind][1].at[flip(s, m), :, window(flip(t, k - bit), width)]
        return remote(block, block, st.at[kind, m, k], rt.at[kind, m, k], (s, flip(t, bit)))

    seen = set()

    def forward(m):
        for kind in range(2):
            for k in relays_of(n_tp):
                before = k - low_bit(k)
                if (kind, m, before) not in seen:
                    share(kind, m, before).wait_recv()
                    seen.add((kind, m, before))
                share(kind, m, k).start()

    for kind in range(2):
        own(kind).start()
    for m in range(1, n_sp):
        for kind in range(2):
            to_expert(kind, m).start()
    for m in range(n_sp):
        for kind in range(2):
            if m == 0:
                own(kind).wait()
            else:
                to_expert(kind, m).wait_recv()
            for bit in bits_of(n_tp):
                share(kind, m, bit).start()
        if m > 0:
            forward(m - 1)
    forward(n_sp - 1)
    for kind in range(2):
        for m in range(n_sp):
            if m > 0:
                to_expert(kind, m).wait_send()
            for k in range(1, n_tp):
                share(kind, m, k).wait_send()
                if (kind, m, k) not in seen:
                    share(kind, m, k).wait_recv()


def combine_kernel(
    n_sp, n_tp, part, mixed, base, pick, out, mixed_all, half, xsend, xrecv, back, ret,
    own_sem, sh, rh, sx, rx, sb, rb, sg, rg, st, rt,
):
    s, t = lax.axis_index("sp"), lax.axis_index("tp")
    width = ret.shape[-1]
    pair, across = flip(t, 1), flip(t, 2)
    greet(
        [(flip(s, m), t) for m in range(1, n_sp)] + [(s, flip(t, b)) for b in bits_of(n_tp)]
    )

    def to_pair(slot):
        chunk = flip(pair, 2) if slot == 0 else pair
        return remote(
            part.at[:, :, window(chunk, width)], half.at[slot], sh.at[slot], rh.at[slot], (s, pair)
        )

    def cross(m):
        q = flip(s, m)
        return remote(xsend.at[q], xrecv.at[q], sx.at[m], rx.at[m], (s, across))

    def give(m):
        q = flip(s, m)
        return remote(back.at[q], ret.at[s], sb.at[m], rb.at[m], (q, t))

    def gather(k):
        bit = low_bit(k)
        block = flip(s, k - bit)
        source = mixed if k == bit else mixed_all.at[block]
        return remote(source, mixed_all.at[block], sg.at[k], rg.at[k], (flip(s, bit), t))

    seen = set()

    def forward(masks):
        for k in masks:
            before = k - low_bit(k)
            if before not in seen:
                gather(before).wait_recv()
                seen.add(before)
            gather(k).start()

    to_pair(0).start()
    to_pair(1).start()
    own = pltpu.make_async_copy(mixed, mixed_all.at[s], own_sem)
    own.start()
    for bit in bits_of(n_sp):
        gather(bit).start()
    order = list(range(n_sp - 1, -1, -1))
    to_pair(0).wait_recv()
    for m in order:
        q = flip(s, m)
        xsend[q] = (
            part[q, :, window(across, width)].astype(jnp.float32) + half[0, q].astype(jnp.float32)
        ).astype(jnp.bfloat16)
        cross(m).start()
    to_pair(1).wait_recv()
    relays = relays_of(n_sp)
    early = [k for k in relays if bin(k).count("1") == 2]
    forward(early)
    for place, m in enumerate(order):
        q = flip(s, m)
        cross(m).wait_recv()
        total = (
            part[q, :, window(t, width)].astype(jnp.float32)
            + half[1, q].astype(jnp.float32)
            + xrecv[q].astype(jnp.float32)
        ).astype(jnp.bfloat16)
        if m == 0:
            ret[s] = total
        else:
            back[q] = total
            give(m).start()
        if place == n_sp // 2:
            forward([k for k in relays if k not in early])
    total = base[...].astype(jnp.float32)
    for m in range(n_sp):
        q = flip(s, m)
        if m > 0:
            give(m).wait_recv()
        total = total + contract_rows(pick[q], ret[q])
    out[:, window(t, width)] = total.astype(jnp.bfloat16)

    def share(k):
        bit = low_bit(k)
        block = out.at[:, window(flip(t, k - bit), width)]
        return remote(block, block, st.at[k], rt.at[k], (s, flip(t, bit)))

    for bit in bits_of(n_tp):
        share(bit).start()
    shared = set()
    for k in relays_of(n_tp):
        before = k - low_bit(k)
        if before not in shared:
            share(before).wait_recv()
            shared.add(before)
        share(k).start()
    for k in range(1, n_tp):
        share(k).wait_send()
        if k not in shared:
            share(k).wait_recv()
    own.wait()
    for slot in range(2):
        to_pair(slot).wait_send()
    for m in range(n_sp):
        cross(m).wait_send()
        if m > 0:
            give(m).wait_send()
            gather(m).wait_send()
            if m not in seen:
                gather(m).wait_recv()


def scan_kernel(
    n_sp, flipped, drive, decay, state_grad, pieces, weight, carry, carries,
    own_sem, sa, ra, sc, rc,
):
    s, t = lax.axis_index("sp"), lax.axis_index("tp")
    rows = drive.shape[0]
    share = flipped.shape[0] // n_sp
    greet([(flip(s, m), t) for m in range(1, n_sp)])

    def piece(m):
        q = flip(s, m)
        return remote(
            flipped.at[window(q, share)], pieces.at[:, window(s, rows)], sa.at[m], ra.at[m], (q, t)
        )

    def send_carry(m):
        return remote(carry, carries.at[s], sc.at[m], rc.at[m], (flip(s, m), t))

    own = pltpu.make_async_copy(
        flipped.at[window(s, share)], pieces.at[:, window(s, rows)], own_sem
    )
    own.start()

    def lap(step, held):
        grad, product = held
        row = rows - 1 - step
        grad = drive[pl.ds(row, 1), :] + grad
        product_here = product
        state_grad[pl.ds(row, 1), :] = grad
        weight[pl.ds(row, 1), :] = product_here
        now = decay[pl.ds(row, 1), :]
        return (now * grad, now * product_here)

    zero = jnp.zeros((1, drive.shape[1]), jnp.float32)
    start, span = lax.fori_loop(0, rows, lap, (zero, zero + 1.0), unroll=8)
    carry[0:1, :] = span
    carry[1:2, :] = start
    for m in range(1, n_sp):
        send_carry(m).start()
    for m in range(1, n_sp):
        piece(m).start()
    for m in range(1, n_sp):
        send_carry(m).wait_recv()
    incoming = zero
    for later in range(n_sp - 1, 0, -1):
        longer = carries[later, 1:2, :] + carries[later, 0:1, :] * incoming
        incoming = jnp.where(later > s, longer, incoming)
    state_grad[...] = state_grad[...] + weight[...] * incoming
    own.wait()
    for m in range(1, n_sp):
        send_carry(m).wait_send()
        piece(m).wait_send()
        piece(m).wait_recv()


def silu_parts(values):
    sig = jax.nn.sigmoid(values)
    return (values * sig, sig * (1.0 + values * (1.0 - sig)))


def route_slots(route_block, experts, capacity):
    flat_ids = route_block.reshape(-1)
    onehot = (flat_ids[:, None] == jnp.arange(experts, dtype=jnp.int32)[None, :]).astype(jnp.int32)
    before = jnp.cumsum(onehot, axis=0) - onehot
    slot_rank = jnp.sum(before * onehot, axis=1)
    return flat_ids * capacity + slot_rank


def contract_rows(left, right):
    return lax.dot_general(
        left, right, (((0,), (0,)), ((), ())), preferred_element_type=jnp.float32
    )


def sparse_body(
    cotangent,
    mixer_out,
    route_ids,
    route_weights,
    conv_out,
    recur_gate,
    input_gate,
    gate_pre,
    states_before,
    decay_rate,
    out_proj,
    recur_map,
    input_map,
    expert_gate,
    expert_up,
    expert_down,
):
    row_count = cotangent.shape[0]
    experts = lax.axis_size("sp")
    capacity = 4 * row_count // experts
    slot_pos = route_slots(route_ids, experts, capacity).reshape(row_count, 2)
    slot_range = jnp.arange(experts * capacity, dtype=jnp.int32)[:, None]
    hit_first = slot_range == slot_pos[None, :, 0]
    hit_second = slot_range == slot_pos[None, :, 1]
    dispatch = (hit_first | hit_second).astype(jnp.bfloat16)
    slot_weight = jnp.sum(
        jnp.where(hit_first, route_weights[None, :, 0], 0.0)
        + jnp.where(hit_second, route_weights[None, :, 1], 0.0),
        axis=1,
    )
    send_rows = jnp.dot(dispatch, mixer_out, preferred_element_type=jnp.float32).astype(
        jnp.bfloat16
    )
    send_cot = (
        jnp.dot(dispatch, cotangent, preferred_element_type=jnp.float32) * slot_weight[:, None]
    ).astype(jnp.bfloat16)
    tps = lax.axis_size("tp")
    features = tps * cotangent.shape[1]
    slots = experts * capacity
    blocks = (experts, capacity, features)
    got_rows, got_cot = call(
        functools.partial(dispatch_kernel, experts, tps),
        [jax.ShapeDtypeStruct(blocks, jnp.bfloat16)] * 2,
        [
            DMA((2,)),
            DMA((2, experts)),
            DMA((2, experts)),
            DMA((2, experts, tps)),
            DMA((2, experts, tps)),
        ],
        0,
        send_rows.reshape(experts, capacity, -1),
        send_cot.reshape(experts, capacity, -1),
    )
    got_rows, got_cot = (got_rows.reshape(slots, features), got_cot.reshape(slots, features))
    w_gate = expert_gate[0]
    w_up = expert_up[0]
    w_down = expert_down[0]
    pre_gate = jnp.dot(got_rows, w_gate, preferred_element_type=jnp.float32)
    pre_up = jnp.dot(got_rows, w_up, preferred_element_type=jnp.float32)
    gate_act, slope = silu_parts(pre_gate)
    active = (gate_act * pre_up).astype(jnp.bfloat16)
    d_active = lax.dot_general(
        got_cot, w_down, (((1,), (1,)), ((), ())), preferred_element_type=jnp.float32
    )
    grad_down = contract_rows(active, got_cot).astype(jnp.bfloat16)
    d_gate = (d_active * pre_up * slope).astype(jnp.bfloat16)
    d_up = (d_active * gate_act).astype(jnp.bfloat16)
    grad_gate = contract_rows(got_rows, d_gate).astype(jnp.bfloat16)
    grad_up = contract_rows(got_rows, d_up).astype(jnp.bfloat16)
    partial_grad = lax.dot_general(
        d_gate, w_gate, (((1,), (1,)), ((), ())), preferred_element_type=jnp.float32
    ) + lax.dot_general(d_up, w_up, (((1,), (1,)), ((), ())), preferred_element_type=jnp.float32)
    channels = conv_out.shape[1]
    rate = decay_rate[None, :]
    recur_f = recur_gate.astype(jnp.float32)
    input_f = input_gate.astype(jnp.float32)
    conv_f = conv_out.astype(jnp.float32)
    before_f = states_before.astype(jnp.float32)
    log_decay = -8.0 * recur_f * rate
    decay_now = jnp.exp(log_decay)
    position = lax.axis_index("sp") * row_count + jnp.arange(row_count, dtype=jnp.int32)
    at_start = (position == 0)[:, None]
    norm_factor = jnp.where(at_start, 1.0, jnp.sqrt(-jnp.expm1(2.0 * log_decay)))
    norm_slope = jnp.where(at_start, 0.0, -jnp.exp(2.0 * log_decay) / norm_factor)
    drive = input_f * conv_f
    state = decay_now * before_f + norm_factor * drive
    gate, gelu_back = jax.vjp(jax.nn.gelu, gate_pre.astype(jnp.float32))
    mixed = (state * gate).astype(jnp.bfloat16)
    block = (experts, capacity, cotangent.shape[1])
    pair_sems, own_sems = (DMA((2,)), DMA((experts,)))
    tp_sems = DMA((tps,))
    out_grad, mixed_all = call(
        functools.partial(combine_kernel, experts, tps),
        [
            jax.ShapeDtypeStruct((row_count, features), jnp.bfloat16),
            jax.ShapeDtypeStruct((experts, row_count, channels), jnp.bfloat16),
        ],
        [
            pltpu.VMEM((2, *block), jnp.bfloat16),
            pltpu.VMEM(block, jnp.bfloat16),
            pltpu.VMEM(block, jnp.bfloat16),
            pltpu.VMEM(block, jnp.bfloat16),
            pltpu.VMEM(block, jnp.bfloat16),
            DMA,
            pair_sems,
            pair_sems,
            *([own_sems] * 6),
            tp_sems,
            tp_sems,
        ],
        1,
        partial_grad.astype(jnp.bfloat16).reshape(blocks),
        mixed,
        cotangent,
        dispatch.reshape(experts, capacity, row_count),
    )
    d_mixed = jnp.dot(out_grad, out_proj, preferred_element_type=jnp.float32)
    state_grad, pieces = call(
        functools.partial(scan_kernel, experts),
        [
            jax.ShapeDtypeStruct((row_count, channels), jnp.float32),
            jax.ShapeDtypeStruct((features // experts, experts * row_count), jnp.bfloat16),
        ],
        [
            pltpu.VMEM((row_count, channels), jnp.float32),
            pltpu.VMEM((2, channels), jnp.float32),
            pltpu.VMEM((experts, 2, channels), jnp.float32),
            DMA,
            *([own_sems] * 4),
        ],
        2,
        out_grad.T,
        d_mixed * gate,
        decay_now,
    )
    grad_out_proj = jnp.dot(
        pieces,
        mixed_all.reshape(experts * row_count, channels),
        preferred_element_type=jnp.float32,
    )
    grad_gate_pre = gelu_back(d_mixed * state)[0].astype(jnp.bfloat16)
    d_log = state_grad * (decay_now * before_f + norm_slope * drive)
    d_recur_pre = (d_log * (-8.0 * rate) * recur_f * (1.0 - recur_f)).astype(jnp.bfloat16)
    d_input_pre = (state_grad * norm_factor * conv_f * input_f * (1.0 - input_f)).astype(
        jnp.bfloat16
    )
    groups = recur_map.shape[0]
    width = recur_map.shape[1]
    through_recur = jnp.einsum(
        "tbj,bij->tbi",
        d_recur_pre.reshape(row_count, groups, width),
        recur_map,
        preferred_element_type=jnp.float32,
    )
    through_input = jnp.einsum(
        "tbj,bij->tbi",
        d_input_pre.reshape(row_count, groups, width),
        input_map,
        preferred_element_type=jnp.float32,
    )
    grad_conv = (
        state_grad * norm_factor * input_f
        + (through_recur + through_input).reshape(row_count, channels)
    ).astype(jnp.bfloat16)
    return (
        grad_gate[None],
        grad_up[None],
        grad_down[None],
        grad_out_proj,
        grad_conv,
        grad_gate_pre,
    )


def body(
    cotangent,
    mixer_out,
    route_ids,
    route_weights,
    conv_out,
    recur_gate,
    input_gate,
    gate_pre,
    states_before,
    decay_rate,
    out_proj,
    recur_map,
    input_map,
    expert_gate,
    expert_up,
    expert_down,
):
    experts, tps = lax.axis_size("sp"), lax.axis_size("tp")
    row_count = cotangent.shape[0]
    capacity = 4 * row_count // experts
    if 2 * capacity < row_count:
        return sparse_body(
            cotangent,
            mixer_out,
            route_ids,
            route_weights,
            conv_out,
            recur_gate,
            input_gate,
            gate_pre,
            states_before,
            decay_rate,
            out_proj,
            recur_map,
            input_map,
            expert_gate,
            expert_up,
            expert_down,
        )
    grad_out_proj, grad_gate, grad_up, grad_down, grad_conv, grad_gate_pre = run_dense(
        experts,
        tps,
        capacity,
        mixer_out,
        cotangent,
        route_ids.T,
        route_weights.T,
        conv_out,
        recur_gate,
        input_gate,
        gate_pre,
        states_before,
        decay_rate[None, :],
        out_proj,
        expert_gate[0],
        expert_up[0],
        expert_down[0],
        recur_map,
        input_map,
    )
    return (
        grad_gate[None],
        grad_up[None],
        grad_down[None],
        grad_out_proj,
        grad_conv,
        grad_gate_pre,
    )


def solution(mesh):
    placed = (
        P("sp", "tp"),
        P("sp", "tp"),
        P("sp", None),
        P("sp", None),
        P("sp", "tp"),
        P("sp", "tp"),
        P("sp", "tp"),
        P("sp", "tp"),
        P("sp", "tp"),
        P("tp"),
        P(None, "tp"),
        P("tp", None, None),
        P("tp", None, None),
        P("sp", None, "tp"),
        P("sp", None, "tp"),
        P("sp", "tp", None),
    )
    return jax.shard_map(
        body,
        mesh=mesh,
        in_specs=placed,
        out_specs=(
            P("sp", None, "tp"),
            P("sp", None, "tp"),
            P("sp", "tp", None),
            P("sp", "tp"),
            P("sp", "tp"),
            P("sp", "tp"),
        ),
        check_vma=False,
    )
```
